512 devices in a mesh: fs: 64 (over z, y), tp: 8 (over x, core).
Axes of the slice: x: 4, y: 8, z: 8, core: 2. Of those that a mesh axis runs over, the one named last changes fastest.
Arguments:
- tokens: bfloat16 [49152, 2048], P('fs'), may hold values from -6 to 6
- norm_gain: float32 [2048], replicated, may hold values from 0.1 to 1.9
- gate_weight: float32 [2048, 5632], P('fs', 'tp'), may hold values from -0.125 to 0.125
- up_weight: float32 [2048, 5632], P('fs', 'tp'), may hold values from -0.125 to 0.125
- gate_scale: float32 [5632], P('tp'), may hold values from 0.1 to 1.9
- up_scale: float32 [5632], P('tp'), may hold values from 0.1 to 1.9
- down_weight: float32 [5632, 2048], P('tp', 'fs'), may hold values from -0.078125 to 0.078125
- down_scale: float32 [2048], P('tp'), may hold values from 0.1 to 1.9
Outputs:
- mixed: bfloat16 [49152, 2048], P('fs', 'tp')
The draws below stay inside these ranges and needn't reach their ends.
All inputs are finite; a program needn't handle non-finite values.
Results may differ from the reference program's by a relative error of at most 0.014.
Values may be sent and summed in bfloat16 or wider, within the bound.
A program may use at most 64 MiB of HBM per device.

```python
import jax
import jax.numpy as jnp
from jax import lax

D = 2048
FF = 5632
TOK_DEV = 768
TOKENS = 49152
N_FS = 64
N_TP = 8


def level_of(key, shape, cuts, low, high):
    loudness, own = 1.0, jax.random.fold_in(key, 6)
    for position, shards_of in cuts:
        draws = jnp.exp(jax.random.uniform(jax.random.fold_in(own, position), (shards_of,), jnp.float32, low / len(cuts), high / len(cuts)))
        loudness = loudness * jnp.repeat(draws, shape[position] // shards_of).reshape([-1 if axis == position else 1 for axis in range(len(shape))])
    return loudness


def centred(own_key, dims, spread, most, split=(), held_as=jnp.bfloat16):
    drawn = spread * jax.random.normal(own_key, dims, jnp.float32)
    if split:
        drawn = drawn * level_of(own_key, dims, split, -0.22, 0.18)
    return jnp.clip(drawn, -most, most).astype(held_as)


def setup_inputs(seed: int = 0) -> dict:
    arg_keys = jax.random.split(jax.random.key(seed), 9)
    return {
        "tokens": centred(arg_keys[0], (TOKENS, D), 1.0, 6.0, ((0, 64),)),
        "norm_gain": jnp.clip(1.0 + 0.18 * jax.random.normal(arg_keys[1], (D,), jnp.float32), 0.1, 1.9),
        "gate_weight": centred(arg_keys[2], (D, FF), D ** -0.5, 0.125, ((0, 64), (1, 8)), jnp.float32),
        "up_weight": centred(arg_keys[3], (D, FF), D ** -0.5, 0.125, ((0, 64), (1, 8)), jnp.float32),
        "gate_scale": jnp.clip(1.0 + 0.18 * jax.random.normal(arg_keys[4], (FF,), jnp.float32), 0.1, 1.9),
        "up_scale": jnp.clip(1.0 + 0.18 * jax.random.normal(arg_keys[5], (FF,), jnp.float32), 0.1, 1.9),
        "down_weight": centred(arg_keys[6], (FF, D), FF ** -0.5, 0.078125, ((0, 8), (1, 64)), jnp.float32),
        "down_scale": jnp.clip(1.0 + 0.18 * jax.random.normal(arg_keys[7], (D,), jnp.float32), 0.1, 1.9),
    }


def reference(tokens, norm_gain, gate_weight, up_weight, gate_scale, up_scale, down_weight, down_scale):
    gate_low = gate_weight.astype(jnp.bfloat16)
    up_low = up_weight.astype(jnp.bfloat16)
    down_low = down_weight.astype(jnp.bfloat16).reshape(N_TP, FF // N_TP, D)

    def one_block(rows):
        values = rows.astype(jnp.float32)
        normed = (values * lax.rsqrt(lax.optimization_barrier(jnp.mean(values * values, axis=-1, keepdims=True)) + 1e-06) * norm_gain).astype(jnp.bfloat16)
        gate = jnp.dot(normed, gate_low, preferred_element_type=jnp.float32) * gate_scale
        up = jnp.dot(normed, up_low, preferred_element_type=jnp.float32) * up_scale
        hidden = (jax.nn.silu(gate) * up).astype(jnp.bfloat16).reshape(rows.shape[0], N_TP, FF // N_TP)
        total = jnp.zeros((rows.shape[0], D), jnp.float32)
        for block in range(N_TP):
            partial_sum = jnp.dot(hidden[:, block], down_low[block], preferred_element_type=jnp.float32).astype(jnp.bfloat16)
            partial_sum = lax.optimization_barrier(partial_sum)
            total = total + partial_sum.astype(jnp.float32)
        return (total * down_scale).astype(jnp.bfloat16)
    blocks = lax.map(one_block, tokens.reshape(N_FS, TOK_DEV, D))
    return blocks.reshape(TOKENS, D)
```

```python
import jax
import jax.numpy as jnp
from jax import lax
from jax.experimental import pallas as pl
from jax.experimental.pallas import tpu as pltpu
from jax.sharding import Mesh
from jax.sharding import PartitionSpec as P

FS = ("fs_0", "fs_1")
MESH = pl.DeviceIdType.MESH
F32, BF16 = jnp.float32, jnp.bfloat16
OFF = (0, 1, -1, 2, -2, 3, -3, 4)
PLUS, MINUS = 0, 1


def wrap(i):
    return lax.rem(i + 16, 8)


class Gather:
    def __init__(self, buf, major_axis, minor_axis, major, minor, sems):
        self.buf, self.major_axis, self.minor_axis = buf, major_axis, minor_axis
        self.major, self.minor = major, minor
        self.send1, self.send2, self.recv1, self.recv2 = sems

    def first(self, way, step, source):
        at = self.buf.at[self.major, wrap(self.minor + source)]
        to = wrap(self.minor + (1 if way == PLUS else -1))
        return pltpu.make_async_remote_copy(
            src_ref=at, dst_ref=at, send_sem=self.send1, recv_sem=self.recv1.at[way, step - 1],
            device_id={self.minor_axis: to}, device_id_type=MESH,
        )

    def second(self, way, hop, j, source):
        at = self.buf.at[wrap(self.major + source), wrap(self.minor + OFF[j])]
        to = wrap(self.major + (1 if way == PLUS else -1))
        return pltpu.make_async_remote_copy(
            src_ref=at, dst_ref=at, send_sem=self.send2, recv_sem=self.recv2.at[way, hop - 1, j],
            device_id={self.major_axis: to}, device_id_type=MESH,
        )

    def start_first(self):
        self.first(PLUS, 1, 0).start()
        self.first(MINUS, 1, 0).start()

    def start_second(self, j):
        self.second(PLUS, 1, j, 0).start()
        self.second(MINUS, 1, j, 0).start()

    def line(self, step):
        self.first(PLUS, step, -step).wait_recv()
        if step < 4:
            self.first(PLUS, step + 1, -step).start()
            self.first(MINUS, step, step).wait_recv()
        if step < 3:
            self.first(MINUS, step + 1, step).start()

    def hop(self, hop, j):
        for way, side, last in ((PLUS, -1, j < 4), (MINUS, 1, j >= 4)):
            self.second(way, hop, j, side * hop).wait_recv()
            if last:
                self.second(way, hop + 1, j, side * hop).start()
            else:
                @pl.when(hop < 3)
                def _():
                    self.second(way, hop + 1, j, side * hop).start()

    def last(self, j):
        if j < 4:
            self.second(PLUS, 4, j, -4).wait_recv()
        else:
            self.second(MINUS, 4, j, 4).wait_recv()

    def drain(self):
        one = self.buf.at[0, pl.ds(0, 7)]
        many = self.buf.at[pl.ds(0, 7)]
        for ref, sem in ((one, self.send1), (many, self.send2)):
            pltpu.make_async_copy(ref, ref, sem).wait()


def kernel(
    tokens, gain, gate_w, up_w, gate_s, up_s, down_w, down_s, out,
    tok, x_a, x_b, buf_a, buf_b, buf_c, buf_d, acc_a, acc_b, hid,
    own_a, own_b, give_a, give_b, got_a, got_b, sum_a, sum_b, all_a, all_b, flat,
    tok_sem, send1, send2, recv1, recv2, pair_send, pair_a, pair_b, x_send, x_a_sem, x_b_sem,
):
    z, y, tp = lax.axis_index("fs_0"), lax.axis_index("fs_1"), lax.axis_index("tp")
    core = lax.rem(tp, 2)
    other = 1 - core
    peer = tp + 1 - 2 * core

    fetch = pltpu.make_async_copy(tokens, tok, tok_sem)
    fetch.start()

    barrier = pltpu.get_barrier_semaphore()
    for axis, me in (("fs_0", z), ("fs_1", y)):
        for side in (1, -1):
            pl.semaphore_signal(barrier, inc=1, device_id={axis: wrap(me + side)}, device_id_type=MESH)
    for k in range(1, 8):
        pl.semaphore_signal(barrier, inc=1, device_id={"tp": lax.rem(tp + k, 8)}, device_id_type=MESH)

    gw, uw = gate_w[...].astype(BF16), up_w[...].astype(BF16)
    tails = jnp.concatenate([gw[:, 640:], uw[:, 640:]], axis=1)
    buf_a[z, y, :, 0:640] = gw[:, 0:640]
    buf_a[z, y, :, 640:768] = uw[:, 0:128]
    buf_b[y, z, :, 0:512] = uw[:, 128:640]
    buf_b[y, z, :, 512:640] = tails

    def sems(k):
        return send1.at[k], send2.at[k], recv1.at[k], recv2.at[k]

    ga = Gather(buf_a, "fs_0", "fs_1", z, y, sems(0))
    gb = Gather(buf_b, "fs_1", "fs_0", y, z, sems(1))
    gc = Gather(buf_c, "fs_0", "fs_1", z, y, sems(2))
    gd = Gather(buf_d, "fs_1", "fs_0", y, z, sems(3))
    wide, deep = (ga, gb), (gc, gd)

    pl.semaphore_wait(barrier, 11)
    for g in wide:
        g.start_first()
    for g in wide:
        g.start_second(0)

    eye = (lax.broadcasted_iota(jnp.int32, (32, 32), 0) == lax.broadcasted_iota(jnp.int32, (32, 32), 1)).astype(BF16)
    turned = lax.dot_general(
        eye, down_w[...].astype(BF16), (((1,), (1,)), ((), ())), preferred_element_type=F32
    )
    turned = jnp.concatenate([turned, jnp.zeros((32, 64), F32)], axis=1).astype(BF16)
    buf_c[z, y] = turned[0:16]
    buf_d[y, z] = turned[16:32]

    acc_a[...] = jnp.zeros_like(acc_a)
    acc_b[...] = jnp.zeros_like(acc_b)
    fetch.wait()

    def prepare(k, _):
        rows = pl.ds(pl.multiple_of(k * 64, 64), 64)
        values = tok[rows, :].astype(F32)
        normed = values * lax.rsqrt(jnp.mean(values * values, axis=-1, keepdims=True) + 1e-06) * gain[...]
        for b in range(8):
            x_a[b, rows, :] = normed[:, b * 256 : b * 256 + 256].astype(BF16)
        lane = lax.broadcasted_iota(jnp.int32, (64, 128), 1) // 32
        for yy in range(8):
            for zh in range(2):
                tile = None
                for zl in range(4):
                    t = (zh * 4 + zl) * 2 + yy // 4
                    piece = normed[:, t * 128 : t * 128 + 128]
                    shift = ((zl - yy % 4) * 32) % 128
                    if shift:
                        piece = pltpu.roll(piece, shift, 1)
                    tile = piece if tile is None else jnp.where(lane == zl, piece, tile)
                x_b[yy, rows, zh * 128 : zh * 128 + 128] = tile.astype(BF16)
        return 0

    for step in range(1, 5):
        for g in wide:
            g.line(step)
        for g in wide:
            g.start_second(2 * step - 1)
            if step < 4:
                g.start_second(2 * step)
        lax.fori_loop((step - 1) * 3, step * 3, prepare, 0)

    for g in deep:
        g.start_first()

    def wide_piece(p, away):
        block, half = p // 2, p % 2
        sign = 1 if block % 2 == 0 else -1
        rows = slice(half * 384, half * 384 + 384)
        if block < 2:
            at = wrap(z + sign * away)
            acc_a[rows, :] += jnp.dot(
                x_a[at, rows, :], buf_a[at].reshape(256, 768), preferred_element_type=F32
            )
        else:
            at = wrap(y + sign * away)
            acc_b[rows, :] += jnp.dot(
                x_b[at, rows, :], buf_b[at].reshape(256, 640), preferred_element_type=F32
            )

    def wide_round(hop, _):
        for j in range(8):
            for g in wide:
                g.hop(hop, j)
            if (j // 2) % 2 == 0:
                wide_piece(j, hop - 1)
            else:
                @pl.when(hop > 1)
                def _():
                    wide_piece(j, hop - 1)
        for step in range(1, 4):
            @pl.when(hop == step)
            def _():
                for g in deep:
                    g.line(step)
        return 0

    lax.fori_loop(1, 4, wide_round, 0)
    for g in deep:
        g.line(4)
    for j in range(8):
        for g in deep:
            g.start_second(j)
    for j in range(8):
        wide_piece(j, 3)
        for g in wide:
            g.last(j)
    for j in (0, 1, 4, 5):
        wide_piece(j, 4)

    def activate(k, _):
        rows = pl.ds(pl.multiple_of(k * 128, 128), 128)
        gate_at, up_at = gate_s[...], up_s[...]
        left, right = acc_a[rows, :], acc_b[rows, :]
        tail = right[:, 512:640]
        g = jnp.concatenate([left[:, 0:640], tail], axis=1) * gate_at
        u = jnp.concatenate([left[:, 640:768], right[:, 0:512], pltpu.roll(tail, 64, 1)], axis=1) * up_at
        h = g / (1.0 + jnp.exp(-g)) * u
        lane = lax.broadcasted_iota(jnp.int32, h.shape, 1)
        h = jnp.where(lane < 704, h, 0.0)
        hid[k] = h.T.astype(BF16)
        return 0

    lax.fori_loop(0, 6, activate, 0)

    def half_of(which):
        return jnp.concatenate([hid[which * 3 + k] for k in range(3)], axis=1)

    def pair(group, at):
        give, got, sem = (give_a, got_a, pair_a) if group == 0 else (give_b, got_b, pair_b)
        return pltpu.make_async_remote_copy(
            src_ref=give.at[at], dst_ref=got.at[at], send_sem=pair_send.at[group], recv_sem=sem.at[at],
            device_id={"tp": peer}, device_id_type=MESH,
        )

    def deep_piece(p, away):
        block, mine = p % 4, p // 4
        sign = 1 if block % 2 == 0 else -1
        group = block // 2
        at = wrap((z, y)[group] + sign * away)
        left = (buf_c, buf_d)[group][at].reshape(128, 768)
        part = jnp.dot(left, half_of(core if mine else other), preferred_element_type=F32)
        if mine:
            (own_a, own_b)[group][at] = part
        else:
            (give_a, give_b)[group][at] = part.astype(BF16)
            pair(group, at).start()

    def to_owner_a(at):
        return pltpu.make_async_remote_copy(
            src_ref=sum_a.at[at], dst_ref=all_a.at[tp], send_sem=x_send.at[0], recv_sem=x_a_sem.at[tp],
            device_id={"tp": at}, device_id_type=MESH,
        )

    def to_owner_b(at, owner):
        return pltpu.make_async_remote_copy(
            src_ref=sum_b.at[at, owner], dst_ref=all_b.at[tp, at], send_sem=x_send.at[1], recv_sem=x_b_sem.at[tp],
            device_id={"tp": owner}, device_id_type=MESH,
        )

    def combine(group, at):
        pair(group, at).wait_recv()
        if group == 0:
            total = (own_a[at] + got_a[at].astype(F32)).astype(BF16).reshape(8, 16, 384)

            @pl.when(at == tp)
            def _():
                all_a[tp] = total

            @pl.when(at != tp)
            def _():
                sum_a[at] = total
                to_owner_a(at).start()
        else:
            sum_b[at] = (own_b[at] + got_b[at].astype(F32)).astype(BF16).reshape(8, 16, 384)
            for k in range(1, 8):
                to_owner_b(at, lax.rem(tp + k, 8)).start()
            all_b[tp, at] = sum_b[at, tp]

    def combine_all(away, both):
        for group, me in ((0, z), (1, y)):
            combine(group, wrap(me + away))
            if both is True:
                combine(group, wrap(me - away))
            elif both is not False:
                @pl.when(both)
                def _():
                    combine(group, wrap(me - away))

    def deep_round(hop, _):
        for j in range(8):
            for g in deep:
                g.hop(hop, j)
            if j % 2 == 0:
                deep_piece(j, hop - 1)
            else:
                @pl.when(hop > 1)
                def _():
                    deep_piece(j, hop - 1)
        combine_all(hop - 1, hop > 1)
        return 0

    lax.fori_loop(1, 4, deep_round, 0)
    for j in range(8):
        for g in deep:
            g.last(j)
        deep_piece(j, 3)
    combine_all(3, True)
    for j in (0, 2, 4, 6):
        deep_piece(j, 4)
    combine_all(4, False)

    for k in range(1, 8):
        source = lax.rem(tp + k, 8)
        pltpu.make_async_copy(all_a.at[source], all_a.at[source], x_a_sem.at[source]).wait()
        pltpu.make_async_copy(all_b.at[source], all_b.at[source], x_b_sem.at[source]).wait()

    for h, held in ((0, all_a), (1, all_b)):
        for c in range(2):
            total = held[c].astype(F32)
            for k in range(1, 4):
                total += held[2 * k + c].astype(F32)
            flat[:, h, :, c * 384 : c * 384 + 384] = total
    scale = down_s[...]
    for k in range(6):
        lanes = slice(k * 128, k * 128 + 128)
        block = flat[:, :, :, lanes].reshape(256, 128)
        out[lanes, :] = (block.T * scale).astype(BF16)

    for g in wide + deep:
        g.drain()
    for group, ref in ((0, give_a), (1, give_b)):
        pltpu.make_async_copy(ref, ref, pair_send.at[group]).wait()
    few = sum_a.at[pl.ds(0, 7)]
    pltpu.make_async_copy(few, few, x_send.at[0]).wait()
    few = sum_b.at[:, pl.ds(0, 7)]
    pltpu.make_async_copy(few, few, x_send.at[1]).wait()


def body(tokens, norm_gain, gate_weight, up_weight, gate_scale, up_scale, down_weight, down_scale):
    def padded(v):
        return jnp.pad(v, (0, 64), constant_values=1.0).reshape(1, 768)

    vmem = pl.BlockSpec(memory_space=pltpu.VMEM)
    hbm = pl.BlockSpec(memory_space=pl.ANY)
    dma = pltpu.SemaphoreType.DMA
    return pl.pallas_call(
        kernel,
        out_shape=jax.ShapeDtypeStruct((768, 256), BF16),
        in_specs=[hbm] + [vmem] * 7,
        out_specs=vmem,
        scratch_shapes=[
            pltpu.VMEM((768, 2048), BF16),
            pltpu.VMEM((8, 768, 256), BF16),
            pltpu.VMEM((8, 768, 256), BF16),
            pltpu.VMEM((8, 8, 32, 768), BF16),
            pltpu.VMEM((8, 8, 32, 640), BF16),
            pltpu.VMEM((8, 8, 16, 768), BF16),
            pltpu.VMEM((8, 8, 16, 768), BF16),
            pltpu.VMEM((768, 768), F32),
            pltpu.VMEM((768, 640), F32),
            pltpu.VMEM((6, 768, 128), BF16),
            pltpu.VMEM((8, 128, 384), F32),
            pltpu.VMEM((8, 128, 384), F32),
            pltpu.VMEM((8, 128, 384), BF16),
            pltpu.VMEM((8, 128, 384), BF16),
            pltpu.VMEM((8, 128, 384), BF16),
            pltpu.VMEM((8, 128, 384), BF16),
            pltpu.VMEM((8, 8, 16, 384), BF16),
            pltpu.VMEM((8, 8, 16, 384), BF16),
            pltpu.VMEM((8, 8, 16, 384), BF16),
            pltpu.VMEM((8, 8, 16, 384), BF16),
            pltpu.VMEM((8, 2, 16, 768), F32),
            dma,
            dma((4,)),
            dma((4,)),
            dma((4, 2, 4)),
            dma((4, 2, 4, 8)),
            dma((2,)),
            dma((8,)),
            dma((8,)),
            dma((2,)),
            dma((8,)),
            dma((8,)),
        ],
        compiler_params=pltpu.CompilerParams(
            collective_id=0, has_side_effects=True, vmem_limit_bytes=56 * 1024 * 1024
        ),
    )(
        tokens, norm_gain.reshape(1, 2048), gate_weight, up_weight, padded(gate_scale), padded(up_scale),
        down_weight, down_scale.reshape(1, 256),
    )


def solution(mesh):
    split = Mesh(mesh.devices.reshape(8, 8, mesh.shape["tp"]), ("fs_0", "fs_1", "tp"))
    placed = (P(FS, None), P(), P(FS, "tp"), P(FS, "tp"), P("tp"), P("tp"), P("tp", FS), P("tp"))
    return jax.shard_map(body, mesh=split, in_specs=placed, out_specs=P(FS, "tp"), check_vma=False)
```

```python
import jax
import jax.numpy as jnp
from jax import lax
from jax.experimental import pallas as pl
from jax.experimental.pallas import tpu as pltpu
from jax.sharding import Mesh
from jax.sharding import PartitionSpec as P

FS = ("fs_0", "fs_1")
MESH = pl.DeviceIdType.MESH
F32, BF16 = jnp.float32, jnp.bfloat16
OFF = (0, 1, -1, 2, -2, 3, -3, 4)
PLUS, MINUS = 0, 1


def wrap(i):
    return lax.rem(i + 16, 8)


class Gather:
    def __init__(self, buf, major, minor, along_major, along_minor, sems):
        self.buf, self.major, self.minor = buf, major, minor
        self.along_major, self.along_minor = along_major, along_minor
        self.send1, self.send2, self.recv1, self.recv2 = sems

    def first(self, way, step, source):
        at = self.buf.at[self.major, wrap(self.minor + source)]
        return pltpu.make_async_remote_copy(
            src_ref=at, dst_ref=at, send_sem=self.send1, recv_sem=self.recv1.at[way, step - 1],
            device_id=self.along_minor[way], device_id_type=MESH,
        )

    def second(self, way, hop, j, source):
        at = self.buf.at[wrap(self.major + source), wrap(self.minor + OFF[j])]
        return pltpu.make_async_remote_copy(
            src_ref=at, dst_ref=at, send_sem=self.send2, recv_sem=self.recv2.at[way, hop - 1, j],
            device_id=self.along_major[way], device_id_type=MESH,
        )

    def start_first(self):
        self.first(PLUS, 1, 0).start()
        self.first(MINUS, 1, 0).start()

    def start_second(self, j):
        self.send(PLUS, j)
        self.send(MINUS, j)

    def send(self, way, j):
        self.second(way, 1, j, 0).start()

    def line(self, step):
        self.first(PLUS, step, -step).wait_recv()
        if step < 4:
            self.first(PLUS, step + 1, -step).start()
            self.first(MINUS, step, step).wait_recv()
        if step < 3:
            self.first(MINUS, step + 1, step).start()

    def hop(self, hop, j):
        for way, side, last in ((PLUS, -1, j < 4), (MINUS, 1, j >= 4)):
            self.second(way, hop, j, side * hop).wait_recv()
            if last or not isinstance(hop, int) or hop < 3:
                self.second(way, hop + 1, j, side * hop).start()

    def last(self, j):
        if j < 4:
            self.second(PLUS, 4, j, -4).wait_recv()
        else:
            self.second(MINUS, 4, j, 4).wait_recv()

    def drain(self):
        one = self.buf.at[0, pl.ds(0, 7)]
        many = self.buf.at[pl.ds(0, 7)]
        for ref, sem in ((one, self.send1), (many, self.send2)):
            pltpu.make_async_copy(ref, ref, sem).wait()


def kernel(
    tokens, gain, gate_w, up_w, gate_s, up_s, down_w, down_s, out,
    tok, gw_in, uw_in, dw_in, x_all, buf_a, buf_b, buf_c, buf_d, acc_a, acc_b, hid,
    own_a, own_b, give_a, give_b, got_a, got_b, sum_a, sum_b, via_a, via_b, all_a, all_b, flat,
    in_sem, send1, send2, recv1, recv2, pair_send, pair_a, pair_b, via_a_sem, via_b_sem, x_send, x_a_sem, x_b_sem,
):
    z, y, tp = lax.axis_index("fs_0"), lax.axis_index("fs_1"), lax.axis_index("tp")
    core = lax.rem(tp, 2)
    other = 1 - core
    peer = tp + 1 - 2 * core
    chip = tp // 2
    onward = 1 - 2 * core

    def place(step, c):
        return 2 * lax.rem(chip + step + 8, 4) + c

    along_z = [(wrap(z + side), y, tp) for side in (1, -1)]
    along_y = [(z, wrap(y + side), tp) for side in (1, -1)]
    barrier = pltpu.get_barrier_semaphore()
    near = along_z + along_y + [(z, y, peer)] + [(z, y, place(step, c)) for step in (1, 3) for c in (0, 1)]
    for device in near:
        pl.semaphore_signal(barrier, inc=1, device_id=device, device_id_type=MESH)

    fetches = [
        pltpu.make_async_copy(src, dst, in_sem.at[k])
        for k, (src, dst) in enumerate(((gate_w, gw_in), (up_w, uw_in), (down_w, dw_in), (tokens, tok)))
    ]
    for fetch in fetches:
        fetch.start()

    major = z + core * (y - z)
    minor = y + core * (z - y)

    def either(first, second):
        return [tuple(f + core * (s - f) for f, s in zip(one, two)) for one, two in zip(first, second)]

    along_major, along_minor = either(along_z, along_y), either(along_y, along_z)

    def sems(k):
        return send1.at[k], send2.at[k], recv1.at[k], recv2.at[k]

    ga = Gather(buf_a, major, minor, along_major, along_minor, sems(0))
    gb = Gather(buf_b, minor, major, along_minor, along_major, sems(1))
    gc = Gather(buf_c, z, y, along_z, along_y, sems(2))
    gd = Gather(buf_d, y, z, along_y, along_z, sems(3))
    wide, deep = (ga, gb), (gc, gd)

    fetches[0].wait()
    fetches[1].wait()
    gw, uw = gw_in[...].astype(BF16), uw_in[...].astype(BF16)
    buf_a[major, minor, :, 0:640] = gw[:, 0:640]
    buf_a[major, minor, :, 640:768] = uw[:, 0:128]
    buf_b[minor, major, :, 0:512] = uw[:, 128:640]
    buf_b[minor, major, :, 512:640] = jnp.concatenate([gw[:, 640:], uw[:, 640:]], axis=1)
    fetches[2].wait()
    turned = jnp.concatenate([dw_in[...], jnp.zeros((32, 64), F32)], axis=1).astype(BF16)
    buf_c[z, y] = turned[0:16]
    buf_d[y, z] = turned[16:32]

    pl.semaphore_wait(barrier, len(near))
    for g in wide + deep:
        g.start_first()
    for g in wide:
        g.start_second(0)

    acc_a[...] = jnp.zeros_like(acc_a)
    acc_b[...] = jnp.zeros_like(acc_b)
    fetches[3].wait()

    def prepare(k, _):
        rows = pl.ds(pl.multiple_of(k * 16, 16), 16)
        values = tok[rows, :].astype(F32)
        normed = values * lax.rsqrt(jnp.mean(values * values, axis=-1, keepdims=True) + 1e-06) * gain[...]
        for b in range(8):
            x_all[0, b, rows, :] = normed[:, b * 256 : b * 256 + 256].astype(BF16)
        lane = lax.broadcasted_iota(jnp.int32, (16, 128), 1) // 32
        for yy in range(8):
            for zh in range(2):
                tile = None
                for zl in range(4):
                    t = (zh * 4 + zl) * 2 + yy // 4
                    piece = normed[:, t * 128 : t * 128 + 128]
                    shift = ((zl - yy % 4) * 32) % 128
                    if shift:
                        piece = pltpu.roll(piece, shift, 1)
                    tile = piece if tile is None else jnp.where(lane == zl, piece, tile)
                x_all[1, yy, rows, zh * 128 : zh * 128 + 128] = tile.astype(BF16)
        return 0

    for step in range(1, 5):
        for g in wide + deep:
            g.line(step)
        for g in wide:
            g.start_second(2 * step - 1)
            if step < 4:
                g.start_second(2 * step)
        lax.fori_loop((step - 1) * 12, step * 12, prepare, 0)

    def wide_piece(p, away):
        block, half = p // 2, p % 2
        sign = 1 if block % 2 == 0 else -1
        rows = slice(half * 384, half * 384 + 384)
        if block < 2:
            at = wrap(major + sign * away)
            acc_a[rows, :] += jnp.dot(
                x_all[core, at, rows, :], buf_a[at].reshape(256, 768), preferred_element_type=F32
            )
        else:
            at = wrap(minor + sign * away)
            acc_b[rows, :] += jnp.dot(
                x_all[other, at, rows, :], buf_b[at].reshape(256, 640), preferred_element_type=F32
            )

    def wide_round(hop, _):
        for j in range(8):
            for g in wide:
                g.hop(hop, j)
            if (j // 2) % 2 == 0:
                wide_piece(j, hop - 1)
            else:
                @pl.when(hop > 1)
                def _():
                    wide_piece(j, hop - 1)
        return 0

    lax.fori_loop(1, 3, wide_round, 0)
    for j in range(8):
        for g in wide:
            g.hop(3, j)
        for g in deep:
            for i in (0, 1):
                g.send(MINUS if j < 4 else PLUS, 2 * (j % 4) + i)
        wide_piece(j, 2)
    for j in range(8):
        wide_piece(j, 3)
        for g in wide:
            g.last(j)
    for j, p in enumerate((0, 1, 4, 5)):
        wide_piece(p, 4)
        for g in deep:
            g.hop(1, 2 * j)
            g.hop(1, 2 * j + 1)

    def activate(k, _):
        rows = pl.ds(pl.multiple_of(k * 128, 128), 128)
        gate_at, up_at = (
            jnp.concatenate([v[...].reshape(1, 704), jnp.ones((1, 64), F32)], axis=1) for v in (gate_s, up_s)
        )
        left, right = acc_a[rows, :], acc_b[rows, :]
        tail = right[:, 512:640]
        g = jnp.concatenate([left[:, 0:640], tail], axis=1) * gate_at
        u = jnp.concatenate([left[:, 640:768], right[:, 0:512], pltpu.roll(tail, 64, 1)], axis=1) * up_at
        h = g / (1.0 + jnp.exp(-g)) * u
        lane = lax.broadcasted_iota(jnp.int32, h.shape, 1)
        h = jnp.where(lane < 704, h, 0.0)
        hid[k] = h.T.astype(BF16)
        return 0

    lax.fori_loop(0, 6, activate, 0)

    def half_of(which):
        return jnp.concatenate([hid[which * 3 + k] for k in range(3)], axis=1)

    def pair(group, at):
        give, got, sem = (give_a, got_a, pair_a) if group == 0 else (give_b, got_b, pair_b)
        return pltpu.make_async_remote_copy(
            src_ref=give.at[at], dst_ref=got.at[at], send_sem=pair_send.at[group], recv_sem=sem.at[at],
            device_id={"tp": peer}, device_id_type=MESH,
        )

    def deep_piece(p, away):
        block, mine = p % 4, p // 4
        sign = 1 if block % 2 == 0 else -1
        group = block // 2
        at = wrap((z, y)[group] + sign * away)
        left = (buf_c, buf_d)[group][at].reshape(128, 768)
        part = jnp.dot(left, half_of(core if mine else other), preferred_element_type=F32)
        if mine:
            (own_a, own_b)[group][at] = part
        else:
            (give_a, give_b)[group][at] = part.astype(BF16)
            pair(group, at).start()

    def put(group, src, slot, row, owner):
        dst, sem = (all_a.at[slot, core], x_a_sem) if group == 0 else (all_b.at[slot, core, row], x_b_sem)
        return pltpu.make_async_remote_copy(
            src_ref=src, dst_ref=dst, send_sem=x_send.at[group], recv_sem=sem.at[slot, core],
            device_id=(z, y, owner), device_id_type=MESH,
        )

    def relay(group, src, at):
        dst, sem = ((via_a, via_a_sem), (via_b, via_b_sem))[group]
        return pltpu.make_async_remote_copy(
            src_ref=src, dst_ref=dst.at[at], send_sem=x_send.at[group], recv_sem=sem.at[at],
            device_id=(z, y, place(onward, core)), device_id_type=MESH,
        )

    straight_slot = 1 + other
    added_slot = 1 + core

    def combine(group, at):
        pair(group, at).wait_recv()
        if group == 0:
            total = own_a[at] + got_a[at].astype(F32)
            low = total.astype(BF16).reshape(8, 16, 384)
            step = lax.rem(at // 2 - chip + 4, 4)

            @pl.when(at == tp)
            def _():
                all_a[0, core] = low

            @pl.when(at == peer)
            def _():
                sum_a[at] = low
                put(0, sum_a.at[at], 0, 0, at).start()

            @pl.when(step == 2)
            def _():
                sum_a[at] = low
                relay(0, sum_a.at[at], at).start()

            @pl.when(step == 2 + onward)
            def _():
                sum_a[at] = low
                put(0, sum_a.at[at], straight_slot, 0, at).start()

            @pl.when(step == 2 - onward)
            def _():
                own_a[at] = total
        else:
            total = own_b[at] + got_b[at].astype(F32)
            own_b[at] = total
            sum_b[at] = total.astype(BF16).reshape(8, 16, 384)
            relay(1, sum_b.at[at, pl.ds(place(2, 0), 2)], at).start()
            for c in (0, 1):
                owner = place(-onward, c)
                put(1, sum_b.at[at, owner], straight_slot, at, owner).start()
            put(1, sum_b.at[at, peer], 0, at, peer).start()
            all_b[0, core, at] = sum_b[at, tp]

    def finish(group, at):
        if group == 0:
            @pl.when(lax.rem(at // 2 - chip + 4, 4) == 2 - onward)
            def _():
                relay(0, sum_a.at[at], at).wait_recv()
                sum_a[at] = (own_a[at] + via_a[at].reshape(128, 384).astype(F32)).astype(BF16).reshape(8, 16, 384)
                put(0, sum_a.at[at], added_slot, 0, at).start()
        else:
            first = place(onward, 0)
            relay(1, sum_b.at[at, pl.ds(0, 2)], at).wait_recv()
            rows = pl.ds(pl.multiple_of(first * 16, 32), 32)
            total = own_b[at, rows, :] + via_b[at].reshape(32, 384).astype(F32)
            sum_b[at, pl.ds(first, 2)] = total.astype(BF16).reshape(2, 16, 384)
            for c in (0, 1):
                put(1, sum_b.at[at, first + c], added_slot, at, first + c).start()

    def each(act, away):
        for group, me in ((1, y), (0, z)):
            act(group, wrap(me + away))
            if 0 < away < 4:
                act(group, wrap(me - away))

    for j in range(8):
        for g in deep:
            g.hop(2, j)
        if j < 4:
            deep_piece((0, 2, 4, 6)[j], 0)
        deep_piece(j, 1)
        if j == 6:
            each(combine, 0)
    each(combine, 1)
    for j in range(8):
        for g in deep:
            g.hop(3, j)
        deep_piece(j, 2)
        if j == 3:
            each(finish, 0)
    each(combine, 2)
    each(finish, 1)
    for j in range(8):
        for g in deep:
            g.last(j)
        deep_piece(j, 3)
    each(combine, 3)
    each(finish, 2)
    for j in (0, 2, 4, 6):
        deep_piece(j, 4)
    each(combine, 4)
    each(finish, 3)
    each(finish, 4)

    for slot in range(3):
        for c in range(2):
            for ref, sem in ((all_a, x_a_sem), (all_b, x_b_sem)):
                landed = pltpu.make_async_copy(ref.at[slot, c], ref.at[slot, c], sem.at[slot, c])
                if slot:
                    landed.wait()
                else:
                    pl.when(core != c)(landed.wait)

    for h, held in ((0, all_a), (1, all_b)):
        for c in range(2):
            total = held[0, c].astype(F32) + held[1, c].astype(F32) + held[2, c].astype(F32)
            flat[:, h, :, c * 384 : c * 384 + 384] = total
    scale = down_s[...]
    for k in range(6):
        lanes = slice(k * 128, k * 128 + 128)
        block = flat[:, :, :, lanes].reshape(256, 128)
        out[lanes, :] = (block.T * scale).astype(BF16)

    for g in wide + deep:
        g.drain()
    for group, ref in ((0, give_a), (1, give_b)):
        pltpu.make_async_copy(ref, ref, pair_send.at[group]).wait()
    few = sum_a.at[pl.ds(0, 7)]
    pltpu.make_async_copy(few, few, x_send.at[0]).wait()
    few = sum_b.at[:, pl.ds(0, 7)]
    pltpu.make_async_copy(few, few, x_send.at[1]).wait()


def body(tokens, norm_gain, gate_weight, up_weight, gate_scale, up_scale, down_weight, down_scale):
    vmem = pl.BlockSpec(memory_space=pltpu.VMEM)
    hbm = pl.BlockSpec(memory_space=pl.ANY)
    dma = pltpu.SemaphoreType.DMA
    return pl.pallas_call(
        kernel,
        out_shape=jax.ShapeDtypeStruct((768, 256), BF16),
        in_specs=[hbm, vmem, hbm, hbm, vmem, vmem, hbm, vmem],
        out_specs=vmem,
        scratch_shapes=[
            pltpu.VMEM((768, 2048), BF16),
            pltpu.VMEM((32, 704), F32),
            pltpu.VMEM((32, 704), F32),
            pltpu.VMEM((32, 704), F32),
            pltpu.VMEM((2, 8, 768, 256), BF16),
            pltpu.VMEM((8, 8, 32, 768), BF16),
            pltpu.VMEM((8, 8, 32, 640), BF16),
            pltpu.VMEM((8, 8, 16, 768), BF16),
            pltpu.VMEM((8, 8, 16, 768), BF16),
            pltpu.VMEM((768, 768), F32),
            pltpu.VMEM((768, 640), F32),
            pltpu.VMEM((6, 768, 128), BF16),
            pltpu.VMEM((8, 128, 384), F32),
            pltpu.VMEM((8, 128, 384), F32),
            pltpu.VMEM((8, 128, 384), BF16),
            pltpu.VMEM((8, 128, 384), BF16),
            pltpu.VMEM((8, 128, 384), BF16),
            pltpu.VMEM((8, 128, 384), BF16),
            pltpu.VMEM((8, 8, 16, 384), BF16),
            pltpu.VMEM((8, 8, 16, 384), BF16),
            pltpu.VMEM((8, 8, 16, 384), BF16),
            pltpu.VMEM((8, 2, 16, 384), BF16),
            pltpu.VMEM((3, 2, 8, 16, 384), BF16),
            pltpu.VMEM((3, 2, 8, 16, 384), BF16),
            pltpu.VMEM((8, 2, 16, 768), F32),
            dma((4,)),
            dma((4,)),
            dma((4,)),
            dma((4, 2, 4)),
            dma((4, 2, 4, 8)),
            dma((2,)),
            dma((8,)),
            dma((8,)),
            dma((8,)),
            dma((8,)),
            dma((2,)),
            dma((3, 2)),
            dma((3, 2)),
        ],
        compiler_params=pltpu.CompilerParams(
            collective_id=0, has_side_effects=True, vmem_limit_bytes=56 * 1024 * 1024
        ),
    )(
        tokens, norm_gain.reshape(1, 2048), gate_weight, up_weight, gate_scale, up_scale,
        down_weight.T, down_scale.reshape(1, 256),
    )


def solution(mesh):
    split = Mesh(mesh.devices.reshape(8, 8, mesh.shape["tp"]), ("fs_0", "fs_1", "tp"))
    placed = (P(FS, None), P(), P(FS, "tp"), P(FS, "tp"), P("tp"), P("tp"), P("tp", FS), P("tp"))
    return jax.shard_map(body, mesh=split, in_specs=placed, out_specs=P(FS, "tp"), check_vma=False)
```

```python
import jax
import jax.numpy as jnp
from jax import lax
from jax.experimental import pallas as pl
from jax.experimental.pallas import tpu as pltpu
from jax.sharding import Mesh
from jax.sharding import PartitionSpec as P

FS = ("fs_0", "fs_1")
MESH = pl.DeviceIdType.MESH
F32, BF16 = jnp.float32, jnp.bfloat16
OFF = (0, 1, -1, 2, -2, 3, -3, 4)
PLUS, MINUS = 0, 1
LATE = 4


def wrap(i):
    return lax.rem(i + 16, 8)


class Gather:
    def __init__(self, buf, major, minor, along_major, along_minor, sems):
        self.buf, self.major, self.minor = buf, major, minor
        self.along_major, self.along_minor = along_major, along_minor
        self.send1, self.send2, self.recv1, self.recv2 = sems

    def first(self, way, step, source):
        at = self.buf.at[self.major, wrap(self.minor + source)]
        return pltpu.make_async_remote_copy(
            src_ref=at, dst_ref=at, send_sem=self.send1, recv_sem=self.recv1.at[way, step - 1],
            device_id=self.along_minor[way], device_id_type=MESH,
        )

    def second(self, way, hop, j, source):
        at = self.buf.at[wrap(self.major + source), wrap(self.minor + OFF[j])]
        if hop == 4:
            half = self.buf.shape[2] // 2
            at = at.at[pl.ds(way * half, half)]
        return pltpu.make_async_remote_copy(
            src_ref=at, dst_ref=at, send_sem=self.send2, recv_sem=self.recv2.at[self.number(way, hop, j // 2)],
            device_id=self.along_major[way], device_id_type=MESH,
        )

    def start_first(self):
        self.first(PLUS, 1, 0).start()
        self.first(MINUS, 1, 0).start()

    def send(self, way, j):
        self.second(way, 1, j, 0).start()

    def number(self, way, hop, pair):
        return 8 * (hop - 1) + 4 * way + pair

    def arrive(self, way, hop, pair):
        here = self.buf.at[0, pl.ds(0, 2 if hop < 4 else 1)]
        pltpu.make_async_copy(here, here, self.recv2.at[self.number(way, hop, pair)]).wait()

    def line(self, step):
        self.first(PLUS, step, -step).wait_recv()
        if step < 4:
            self.first(PLUS, step + 1, -step).start()
            self.first(MINUS, step, step).wait_recv()
        if step < 3:
            self.first(MINUS, step + 1, step).start()

    def hop(self, hop, pair):
        for way, side in ((PLUS, -1), (MINUS, 1)):
            self.arrive(way, hop, pair)
            if hop < 4:
                for j in (2 * pair, 2 * pair + 1):
                    self.second(way, hop + 1, j, side * hop).start()

    def drain(self):
        one = self.buf.at[0, pl.ds(0, 7)]
        many = self.buf.at[pl.ds(0, 7)]
        for ref, sem in ((one, self.send1), (many, self.send2)):
            pltpu.make_async_copy(ref, ref, sem).wait()


def kernel(
    tokens, gain, gate_w, up_w, gate_s, up_s, down_w, down_s, out,
    tok, gw_in, uw_in, dw_in, gain_in, gs_in, us_in, ds_in, perm, x_all, buf_a, buf_b, buf_c, buf_d, acc_a, acc_b, hid,
    own_a, own_b, give_a, give_b, got_a, got_b, sum_a, sum_b, via_a, via_b, all_a, all_b, flat,
    in_sem, send1, send2, recv1, recv2, pair_send, pair_a, pair_b, via_a_sem, via_b_sem, x_send, x_a_sem, x_b_sem,
):
    z, y, tp = lax.axis_index("fs_0"), lax.axis_index("fs_1"), lax.axis_index("tp")
    core = lax.rem(tp, 2)
    other = 1 - core
    peer = tp + 1 - 2 * core
    chip = tp // 2
    onward = 1 - 2 * core

    def place(step, c):
        return 2 * lax.rem(chip + step + 8, 4) + c

    along_z = [(wrap(z + side), y, tp) for side in (1, -1)]
    along_y = [(z, wrap(y + side), tp) for side in (1, -1)]
    all_a[3] = jnp.zeros((2, 8, 16, 384), BF16)
    all_b[3] = jnp.zeros((2, 8, 16, 384), BF16)

    barrier = pltpu.get_barrier_semaphore()
    near = along_z + along_y + [(z, y, lax.rem(tp + k, 8)) for k in range(1, 8)]
    for device in near:
        pl.semaphore_signal(barrier, inc=1, device_id=device, device_id_type=MESH)

    inputs = (
        (gate_w, gw_in), (up_w, uw_in), (down_w, dw_in), (tokens, tok), (gain, gain_in), (gate_s, gs_in), (up_s, us_in), (down_s, ds_in),
    )
    fetches = [
        pltpu.make_async_copy(src, dst, in_sem.at[k])
        for k, (src, dst) in enumerate(inputs)
    ]
    for fetch in fetches:
        fetch.start()

    major = z + core * (y - z)
    minor = y + core * (z - y)

    def either(first, second):
        return [tuple(f + core * (s - f) for f, s in zip(one, two)) for one, two in zip(first, second)]

    along_major, along_minor = either(along_z, along_y), either(along_y, along_z)

    def sems(k):
        return send1.at[k], send2.at[k], recv1.at[k], recv2.at[k]

    ga = Gather(buf_a, major, minor, along_major, along_minor, sems(0))
    gb = Gather(buf_b, minor, major, along_minor, along_major, sems(1))
    gc = Gather(buf_c, z, y, along_z, along_y, sems(2))
    gd = Gather(buf_d, y, z, along_y, along_z, sems(3))
    wide, deep = (ga, gb), (gc, gd)

    fetches[0].wait()
    fetches[1].wait()
    gw, uw = gw_in[...].astype(BF16), uw_in[...].astype(BF16)
    buf_a[major, minor, :, 0:640] = gw[:, 0:640]
    buf_a[major, minor, :, 640:768] = uw[:, 0:128]
    buf_b[minor, major, :, 0:512] = uw[:, 128:640]
    buf_b[minor, major, :, 512:640] = jnp.concatenate([gw[:, 640:], uw[:, 640:]], axis=1)
    pl.semaphore_wait(barrier, len(near))
    for g in wide:
        g.start_first()
    for g in wide:
        for way in (PLUS, MINUS):
            g.send(way, 0)
    fetches[2].wait()
    turned = jnp.concatenate([dw_in[...], jnp.zeros((32, 64), F32)], axis=1).astype(BF16)
    buf_c[z, y] = turned[0:16]
    buf_d[y, z] = turned[16:32]
    for g in deep:
        g.start_first()

    for fetch in fetches[3:]:
        fetch.wait()

    def normalize(k, _):
        rows = pl.ds(pl.multiple_of(k * 64, 64), 64)
        squares = jnp.zeros((64, 128), F32)
        for t in range(16):
            v = tok[rows, t * 128 : t * 128 + 128].astype(F32)
            squares += v * v
        factor = lax.rsqrt(jnp.sum(squares, axis=-1, keepdims=True) * (1 / 2048) + 1e-06)
        for t in range(16):
            v = tok[rows, t * 128 : t * 128 + 128].astype(F32) * factor * gain_in[:, t * 128 : t * 128 + 128]
            x_all[0, t // 2, rows, t % 2 * 128 : t % 2 * 128 + 128] = v.astype(BF16)
        return 0

    lax.fori_loop(0, 5, normalize, 0)

    k, n = (lax.broadcasted_iota(jnp.int32, (512, 512), d) for d in (0, 1))
    chosen = (k // 128 == n % 128 // 32) & (k % 128 // 32 == n // 128) & (k % 32 == n % 32)
    perm[...] = chosen.astype(F32).astype(BF16)

    def permute(group):
        zh, yh = group // 2, group % 2

        def some(k, _):
            rows = pl.ds(pl.multiple_of(k * 256, 256), 256)
            source = jnp.concatenate([x_all[0, zh * 4 + zl, rows, yh * 128 : yh * 128 + 128] for zl in range(4)], axis=1)
            moved = jnp.dot(source, perm[...], preferred_element_type=F32).astype(BF16)
            for yq in range(4):
                x_all[1, yh * 4 + yq, rows, zh * 128 : zh * 128 + 128] = moved[:, yq * 128 : yq * 128 + 128]
            return 0

        lax.fori_loop(0, 3, some, 0)

    for step in range(1, 5):
        for g in wide + deep:
            g.line(step)
        for j in (2 * step - 1, 2 * step):
            for g in wide:
                for way in (PLUS, MINUS):
                    if j < 8:
                        g.send(way, j)
        if step < 4:
            lax.fori_loop((5, 8, 10)[step - 1], (8, 10, 12)[step - 1], normalize, 0)
        if step > 1:
            for g in wide:
                g.hop(1, step - 2)
    permute(0)
    permute(1)
    for g in wide:
        g.hop(1, 3)
    permute(2)
    permute(3)
    acc_a[...] = jnp.zeros_like(acc_a)
    acc_b[...] = jnp.zeros_like(acc_b)

    def wide_piece(p, away):
        block, half = p // 2, p % 2
        sign = 1 if block % 2 == 0 else -1
        rows = slice(half * 384, half * 384 + 384)
        if block < 2:
            at = wrap(major + sign * away)
            acc_a[rows, :] += jnp.dot(
                x_all[core, at, rows, :], buf_a[at].reshape(256, 768), preferred_element_type=F32
            )
        else:
            at = wrap(minor + sign * away)
            acc_b[rows, :] += jnp.dot(
                x_all[other, at, rows, :], buf_b[at].reshape(256, 640), preferred_element_type=F32
            )

    for pair in range(4):
        for g in wide:
            g.hop(2, pair)
        wide_piece((0, 1, 4, 5)[pair], 0)
        wide_piece(2 * pair, 1)
        wide_piece(2 * pair + 1, 1)
    for pair in range(4):
        for g in wide:
            g.hop(3, pair)
        wide_piece(2 * pair, 2)
        wide_piece(2 * pair + 1, 2)
    for j in range(8):
        for g in deep:
            for way in (PLUS, MINUS):
                g.send(way, j)
    for pair in range(4):
        wide_piece(2 * pair, 3)
        wide_piece(2 * pair + 1, 3)
        for g in wide:
            g.hop(4, pair)
    for p in (0, 1, 4, 5):
        wide_piece(p, 4)

    def deep_hop(hop, pair):
        for g in deep:
            g.hop(hop, pair)

    deep_hop(1, 0)

    def activate(k, _):
        rows = pl.ds(pl.multiple_of(k * 128, 128), 128)
        gate_at, up_at = (
            jnp.concatenate([v[...].reshape(1, 704), jnp.ones((1, 64), F32)], axis=1) for v in (gs_in, us_in)
        )
        left, right = acc_a[rows, :], acc_b[rows, :]
        tail = right[:, 512:640]
        g = jnp.concatenate([left[:, 0:640], tail], axis=1) * gate_at
        u = jnp.concatenate([left[:, 640:768], right[:, 0:512], pltpu.roll(tail, 64, 1)], axis=1) * up_at
        h = g / (1.0 + jnp.exp(-g)) * u
        lane = lax.broadcasted_iota(jnp.int32, h.shape, 1)
        h = jnp.where(lane < 704, h, 0.0)
        hid[k] = h.T.astype(BF16)
        return 0

    lax.fori_loop(0, 6, activate, 0)

    def half_of(which):
        return jnp.concatenate([hid[which * 3 + k] for k in range(3)], axis=1)

    def exchange(group, at):
        give, got, sem = (give_a, got_a, pair_a) if group == 0 else (give_b, got_b, pair_b)
        return pltpu.make_async_remote_copy(
            src_ref=give.at[at], dst_ref=got.at[at], send_sem=pair_send.at[group], recv_sem=sem.at[at],
            device_id={"tp": peer}, device_id_type=MESH,
        )

    def deep_piece(p, away):
        block, mine = p % 4, p // 4
        sign = 1 if block % 2 == 0 else -1
        group = block // 2
        at = wrap((z, y)[group] + sign * away)
        left = (buf_c, buf_d)[group][at].reshape(128, 768)
        part = jnp.dot(left, half_of(core if mine else other), preferred_element_type=F32)
        if mine:
            (own_a, own_b)[group][at] = part
        else:
            (give_a, give_b)[group][at] = part.astype(BF16)
            exchange(group, at).start()

    def put(group, src, slot, row, owner):
        dst, sem = (all_a.at[slot, core], x_a_sem) if group == 0 else (all_b.at[slot, core, row], x_b_sem)
        return pltpu.make_async_remote_copy(
            src_ref=src, dst_ref=dst, send_sem=x_send.at[group], recv_sem=sem.at[slot, core],
            device_id=(z, y, owner), device_id_type=MESH,
        )

    def relay(group, src, at):
        dst, sem = ((via_a, via_a_sem), (via_b, via_b_sem))[group]
        return pltpu.make_async_remote_copy(
            src_ref=src, dst_ref=dst.at[at], send_sem=x_send.at[group], recv_sem=sem.at[at],
            device_id=(z, y, place(onward, core)), device_id_type=MESH,
        )

    straight_slot = 1 + other
    added_slot = 1 + core

    def combine_one(group, at, late):
        exchange(group, at).wait_recv()
        if group == 0:
            total = own_a[at] + got_a[at].astype(F32)
            low = total.astype(BF16).reshape(8, 16, 384)
            step = lax.rem(at // 2 - chip + 4, 4)

            @pl.when(at == tp)
            def _():
                all_a[0, core] = low

            @pl.when(at != tp)
            def _():
                sum_a[at] = low

            @pl.when(at == peer)
            def _():
                put(0, sum_a.at[at], 0, 0, at).start()

            @pl.when(step == 2)
            def _():
                (put(0, sum_a.at[at], 3, 0, at) if late else relay(0, sum_a.at[at], at)).start()

            @pl.when(step == 2 + onward)
            def _():
                put(0, sum_a.at[at], straight_slot, 0, at).start()

            @pl.when(step == 2 - onward)
            def _():
                if late:
                    put(0, sum_a.at[at], added_slot, 0, at).start()
                else:
                    own_a[at] = total
        else:
            total = own_b[at] + got_b[at].astype(F32)
            sum_b[at] = total.astype(BF16).reshape(8, 16, 384)
            if late:
                for c in (0, 1):
                    put(1, sum_b.at[at, place(2, c)], 3, at, place(2, c)).start()
                for c in (0, 1):
                    put(1, sum_b.at[at, place(onward, c)], added_slot, at, place(onward, c)).start()
            else:
                own_b[at] = total
                relay(1, sum_b.at[at, pl.ds(place(2, 0), 2)], at).start()
            for c in (0, 1):
                put(1, sum_b.at[at, place(-onward, c)], straight_slot, at, place(-onward, c)).start()
            put(1, sum_b.at[at, peer], 0, at, peer).start()
            all_b[0, core, at] = sum_b[at, tp]

    def finish_one(group, at):
        if group == 0:
            @pl.when(lax.rem(at // 2 - chip + 4, 4) == 2 - onward)
            def _():
                relay(0, sum_a.at[at], at).wait_recv()
                sum_a[at] = (own_a[at] + via_a[at].reshape(128, 384).astype(F32)).astype(BF16).reshape(8, 16, 384)
                put(0, sum_a.at[at], added_slot, 0, at).start()
        else:
            first = place(onward, 0)
            relay(1, sum_b.at[at, pl.ds(0, 2)], at).wait_recv()
            rows = pl.ds(pl.multiple_of(first * 16, 32), 32)
            total = own_b[at, rows, :] + via_b[at].reshape(32, 384).astype(F32)
            sum_b[at, pl.ds(first, 2)] = total.astype(BF16).reshape(2, 16, 384)
            for c in (0, 1):
                put(1, sum_b.at[at, first + c], added_slot, at, first + c).start()

    def both_sides(act, away):
        for group, me in ((0, z), (1, y)):
            act(group, wrap(me + away))
            if 0 < away < 4:
                act(group, wrap(me - away))

    def combine(away):
        both_sides(lambda group, at: combine_one(group, at, away >= LATE), away)

    def finish(away):
        both_sides(finish_one, away)

    def deep_pieces(which, away):
        for p in which:
            deep_piece(p, away)

    deep_hop(1, 1)
    deep_pieces((0, 2, 4, 6), 0)
    deep_hop(1, 2)
    combine(0)
    deep_hop(1, 3)
    deep_pieces((0, 1, 2, 3), 1)
    deep_hop(2, 0)
    deep_pieces((4, 5), 1)
    deep_hop(2, 1)
    deep_pieces((6, 7), 1)
    combine(1)
    deep_hop(2, 2)
    deep_hop(2, 3)
    finish(0)
    deep_pieces((0, 1, 2, 3), 2)
    deep_hop(3, 0)
    deep_pieces((4, 5, 6, 7), 2)
    deep_hop(3, 1)
    combine(2)
    deep_hop(3, 2)
    deep_hop(3, 3)
    finish(1)
    deep_pieces((0, 1, 2, 3, 4, 5, 6, 7), 3)
    combine(3)
    finish(2)
    for pair in range(4):
        deep_hop(4, pair)
    deep_pieces((0, 2, 4, 6), 4)
    combine(4)
    finish(3)

    apart = lax.rem(tp - z + 8, 8)
    far_a = (apart >= LATE) & (apart <= 8 - LATE)
    for c in range(2):
        for slot in range(4):
            rows = pl.ds(0, 8 if slot < 3 else 9 - 2 * LATE)
            wait_a = pltpu.make_async_copy(all_a.at[slot, c], all_a.at[slot, c], x_a_sem.at[slot, c]).wait
            wait_b = pltpu.make_async_copy(all_b.at[slot, c, rows], all_b.at[slot, c, rows], x_b_sem.at[slot, c]).wait
            if slot == 0:
                pl.when(core != c)(wait_a)
                pl.when(core != c)(wait_b)
            else:
                if slot < 3:
                    wait_a()
                else:
                    pl.when(far_a)(wait_a)
                wait_b()

    for h, held in ((0, all_a), (1, all_b)):
        for c in range(2):
            total = held[0, c].astype(F32)
            for slot in range(1, 4):
                total += held[slot, c].astype(F32)
            flat[:, h, :, c * 384 : c * 384 + 384] = total
    scale = ds_in[...]
    for k in range(6):
        lanes = slice(k * 128, k * 128 + 128)
        block = flat[:, :, :, lanes].reshape(256, 128)
        out[lanes, :] = (block.T * scale).astype(BF16)

    for g in wide + deep:
        g.drain()
    for group, ref in ((0, give_a), (1, give_b)):
        pltpu.make_async_copy(ref, ref, pair_send.at[group]).wait()
    few = sum_a.at[pl.ds(0, 7)]
    pltpu.make_async_copy(few, few, x_send.at[0]).wait()
    few = sum_b.at[:, pl.ds(0, 7)]
    pltpu.make_async_copy(few, few, x_send.at[1]).wait()


def body(tokens, norm_gain, gate_weight, up_weight, gate_scale, up_scale, down_weight, down_scale):
    vmem = pl.BlockSpec(memory_space=pltpu.VMEM)
    hbm = pl.BlockSpec(memory_space=pl.ANY)
    dma = pltpu.SemaphoreType.DMA
    return pl.pallas_call(
        kernel,
        out_shape=jax.ShapeDtypeStruct((768, 256), BF16),
        in_specs=[hbm] * 8,
        out_specs=vmem,
        scratch_shapes=[
            pltpu.VMEM((768, 2048), BF16),
            pltpu.VMEM((32, 704), F32),
            pltpu.VMEM((32, 704), F32),
            pltpu.VMEM((32, 704), F32),
            pltpu.VMEM((1, 2048), F32),
            pltpu.VMEM((704,), F32),
            pltpu.VMEM((704,), F32),
            pltpu.VMEM((1, 256), F32),
            pltpu.VMEM((512, 512), BF16),
            pltpu.VMEM((2, 8, 768, 256), BF16),
            pltpu.VMEM((8, 8, 32, 768), BF16),
            pltpu.VMEM((8, 8, 32, 640), BF16),
            pltpu.VMEM((8, 8, 16, 768), BF16),
            pltpu.VMEM((8, 8, 16, 768), BF16),
            pltpu.VMEM((768, 768), F32),
            pltpu.VMEM((768, 640), F32),
            pltpu.VMEM((6, 768, 128), BF16),
            pltpu.VMEM((8, 128, 384), F32),
            pltpu.VMEM((8, 128, 384), F32),
            pltpu.VMEM((8, 128, 384), BF16),
            pltpu.VMEM((8, 128, 384), BF16),
            pltpu.VMEM((8, 128, 384), BF16),
            pltpu.VMEM((8, 128, 384), BF16),
            pltpu.VMEM((8, 8, 16, 384), BF16),
            pltpu.VMEM((8, 8, 16, 384), BF16),
            pltpu.VMEM((8, 8, 16, 384), BF16),
            pltpu.VMEM((8, 2, 16, 384), BF16),
            pltpu.VMEM((4, 2, 8, 16, 384), BF16),
            pltpu.VMEM((4, 2, 8, 16, 384), BF16),
            pltpu.VMEM((8, 2, 16, 768), F32),
            dma((8,)),
            dma((4,)),
            dma((4,)),
            dma((4, 2, 4)),
            dma((4, 32)),
            dma((2,)),
            dma((8,)),
            dma((8,)),
            dma((8,)),
            dma((8,)),
            dma((2,)),
            dma((4, 2)),
            dma((4, 2)),
        ],
        compiler_params=pltpu.CompilerParams(
            collective_id=0, has_side_effects=True, vmem_limit_bytes=56 * 1024 * 1024
        ),
    )(
        tokens, norm_gain.reshape(1, 2048), gate_weight, up_weight, gate_scale, up_scale,
        down_weight.T, down_scale.reshape(1, 256),
    )


def solution(mesh):
    split = Mesh(mesh.devices.reshape(8, 8, mesh.shape["tp"]), ("fs_0", "fs_1", "tp"))
    placed = (P(FS, None), P(), P(FS, "tp"), P(FS, "tp"), P("tp"), P("tp"), P("tp", FS), P("tp"))
    return jax.shard_map(body, mesh=split, in_specs=placed, out_specs=P(FS, "tp"), check_vma=False)
```

```python
import jax
import jax.numpy as jnp
from jax import lax
from jax.experimental import pallas as pl
from jax.experimental.pallas import tpu as pltpu
from jax.sharding import Mesh
from jax.sharding import PartitionSpec as P

FS = ("fs_0", "fs_1")
MESH = pl.DeviceIdType.MESH
F32, BF16 = jnp.float32, jnp.bfloat16
OFF = (0, 1, -1, 2, -2, 3, -3, 4)
PLUS, MINUS = 0, 1
WIDE, DEEP = (2, 4, 4, 4), (2, 2, 2, 8)


def wrap(i):
    return lax.rem(i + 16, 8)


class Gather:
    def __init__(self, buf, major, minor, along_major, along_minor, sems, sizes):
        self.buf, self.major, self.minor, self.sizes = buf, major, minor, sizes
        self.along_major, self.along_minor = along_major, along_minor
        self.send1, self.send2, self.recv1, self.recv2 = sems

    def first(self, way, step, source):
        at = self.buf.at[self.major, wrap(self.minor + source)]
        return pltpu.make_async_remote_copy(
            src_ref=at, dst_ref=at, send_sem=self.send1, recv_sem=self.recv1.at[way, step - 1],
            device_id=self.along_minor[way], device_id_type=MESH,
        )

    def second(self, way, hop, j, source):
        at = self.buf.at[wrap(self.major + source), wrap(self.minor + OFF[j])]
        if hop == 4:
            half = self.buf.shape[2] // 2
            at = at.at[pl.ds(way * half, half)]
        return pltpu.make_async_remote_copy(
            src_ref=at, dst_ref=at, send_sem=self.send2, recv_sem=self.recv2.at[self.number(way, hop, j // self.sizes[hop - 1])],
            device_id=self.along_major[way], device_id_type=MESH,
        )

    def start_first(self):
        self.first(PLUS, 1, 0).start()
        self.first(MINUS, 1, 0).start()

    def send(self, way, j):
        self.second(way, 1, j, 0).start()

    def number(self, way, hop, group):
        counts = [8 // size for size in self.sizes]
        return 2 * sum(counts[: hop - 1]) + way * counts[hop - 1] + group

    def arrive(self, way, hop, group):
        size = self.sizes[hop - 1]
        here = self.buf.at[0, pl.ds(0, size if hop < 4 else size // 2)]
        pltpu.make_async_copy(here, here, self.recv2.at[self.number(way, hop, group)]).wait()

    def line(self, step):
        self.first(PLUS, step, -step).wait_recv()
        if step < 4:
            self.first(PLUS, step + 1, -step).start()
            self.first(MINUS, step, step).wait_recv()
        if step < 3:
            self.first(MINUS, step + 1, step).start()

    def hop(self, hop, group):
        size = self.sizes[hop - 1]
        for way, side in ((PLUS, -1), (MINUS, 1)):
            self.arrive(way, hop, group)
            if hop < 4:
                for j in range(group * size, group * size + size):
                    self.second(way, hop + 1, j, side * hop).start()

    def drain(self):
        one = self.buf.at[0, pl.ds(0, 7)]
        many = self.buf.at[pl.ds(0, 7)]
        for ref, sem in ((one, self.send1), (many, self.send2)):
            pltpu.make_async_copy(ref, ref, sem).wait()


def kernel(
    tokens, gain, gate_w, up_w, gate_s, up_s, down_w, down_s, out,
    tok, gw_in, uw_in, dw_in, gain_in, gs_in, us_in, ds_in, perm, x_all, buf_a, buf_b, buf_c, buf_d, acc_a, acc_b, hid,
    own_a, own_b, give_a, give_b, got_a, got_b, sum_a, sum_b, via_a, via_b, all_a, all_b, flat,
    in_sem, send1, send2, recv1, recv2, pair_send, pair_a, pair_b, via_a_sem, via_b_sem, x_send, x_a_sem, x_b_sem,
):
    z, y, tp = lax.axis_index("fs_0"), lax.axis_index("fs_1"), lax.axis_index("tp")
    core = lax.rem(tp, 2)
    other = 1 - core
    peer = tp + 1 - 2 * core
    chip = tp // 2
    onward = 1 - 2 * core

    def place(step, c):
        return 2 * lax.rem(chip + step + 8, 4) + c

    along_z = [(wrap(z + side), y, tp) for side in (1, -1)]
    along_y = [(z, wrap(y + side), tp) for side in (1, -1)]
    barrier = pltpu.get_barrier_semaphore()
    near = along_z + along_y + [(z, y, peer)] + [(z, y, place(step, c)) for step in (1, 3) for c in (0, 1)]
    for device in near:
        pl.semaphore_signal(barrier, inc=1, device_id=device, device_id_type=MESH)

    inputs = (
        (gate_w, gw_in), (up_w, uw_in), (down_w, dw_in), (tokens, tok), (gain, gain_in), (gate_s, gs_in), (up_s, us_in), (down_s, ds_in),
    )
    fetches = [
        pltpu.make_async_copy(src, dst, in_sem.at[k])
        for k, (src, dst) in enumerate(inputs)
    ]
    for fetch in fetches:
        fetch.start()

    major = z + core * (y - z)
    minor = y + core * (z - y)

    def either(first, second):
        return [tuple(f + core * (s - f) for f, s in zip(one, two)) for one, two in zip(first, second)]

    along_major, along_minor = either(along_z, along_y), either(along_y, along_z)

    def sems(k):
        return send1.at[k], send2.at[k], recv1.at[k], recv2.at[k]

    ga = Gather(buf_a, major, minor, along_major, along_minor, sems(0), WIDE)
    gb = Gather(buf_b, minor, major, along_minor, along_major, sems(1), WIDE)
    gc = Gather(buf_c, z, y, along_z, along_y, sems(2), DEEP)
    gd = Gather(buf_d, y, z, along_y, along_z, sems(3), DEEP)
    wide, deep = (ga, gb), (gc, gd)

    fetches[0].wait()
    fetches[1].wait()
    gw, uw = gw_in[...].astype(BF16), uw_in[...].astype(BF16)
    buf_a[major, minor, :, 0:640] = gw[:, 0:640]
    buf_a[major, minor, :, 640:768] = uw[:, 0:128]
    buf_b[minor, major, :, 0:512] = uw[:, 128:640]
    buf_b[minor, major, :, 512:640] = jnp.concatenate([gw[:, 640:], uw[:, 640:]], axis=1)
    pl.semaphore_wait(barrier, len(near))
    for g in wide:
        g.start_first()
    for g in wide:
        for way in (PLUS, MINUS):
            g.send(way, 0)
    fetches[2].wait()
    turned = jnp.concatenate([dw_in[...], jnp.zeros((32, 64), F32)], axis=1).astype(BF16)
    buf_c[z, y] = turned[0:16]
    buf_d[y, z] = turned[16:32]
    for g in deep:
        g.start_first()
    for g in deep:
        for way in (PLUS, MINUS):
            g.send(way, 0)

    for fetch in fetches[3:]:
        fetch.wait()

    def normalize(k, _):
        rows = pl.ds(pl.multiple_of(k * 64, 64), 64)
        squares = jnp.zeros((64, 128), F32)
        for t in range(16):
            v = tok[rows, t * 128 : t * 128 + 128].astype(F32)
            squares += v * v
        factor = lax.rsqrt(jnp.sum(squares, axis=-1, keepdims=True) * (1 / 2048) + 1e-06)
        for t in range(16):
            v = tok[rows, t * 128 : t * 128 + 128].astype(F32) * factor * gain_in[:, t * 128 : t * 128 + 128]
            x_all[0, t // 2, rows, t % 2 * 128 : t % 2 * 128 + 128] = v.astype(BF16)
        return 0

    lax.fori_loop(0, 5, normalize, 0)

    k, n = (lax.broadcasted_iota(jnp.int32, (512, 512), d) for d in (0, 1))
    chosen = (k // 128 == n % 128 // 32) & (k % 128 // 32 == n // 128) & (k % 32 == n % 32)
    perm[...] = chosen.astype(F32).astype(BF16)

    def permute(group):
        zh, yh = group // 2, group % 2

        def some(k, _):
            rows = pl.ds(pl.multiple_of(k * 256, 256), 256)
            source = jnp.concatenate([x_all[0, zh * 4 + zl, rows, yh * 128 : yh * 128 + 128] for zl in range(4)], axis=1)
            moved = jnp.dot(source, perm[...], preferred_element_type=F32).astype(BF16)
            for yq in range(4):
                x_all[1, yh * 4 + yq, rows, zh * 128 : zh * 128 + 128] = moved[:, yq * 128 : yq * 128 + 128]
            return 0

        lax.fori_loop(0, 3, some, 0)

    for step in range(1, 5):
        for g in wide:
            g.line(step)
            for j in (2 * step - 1, 2 * step):
                for way in (PLUS, MINUS):
                    if j < 8:
                        g.send(way, j)
        for g in deep:
            g.line(step)
        if step < 4:
            lax.fori_loop((5, 8, 10)[step - 1], (8, 10, 12)[step - 1], normalize, 0)
        if step > 1:
            for g in wide:
                g.hop(1, step - 2)
    permute(0)
    permute(1)
    for g in wide:
        g.hop(1, 3)
    permute(2)
    permute(3)
    acc_a[...] = jnp.zeros_like(acc_a)
    acc_b[...] = jnp.zeros_like(acc_b)

    def wide_piece(p, away):
        block, half = p // 2, p % 2
        sign = 1 if block % 2 == 0 else -1
        rows = slice(half * 384, half * 384 + 384)
        if block < 2:
            at = wrap(major + sign * away)
            acc_a[rows, :] += jnp.dot(
                x_all[core, at, rows, :], buf_a[at].reshape(256, 768), preferred_element_type=F32
            )
        else:
            at = wrap(minor + sign * away)
            acc_b[rows, :] += jnp.dot(
                x_all[other, at, rows, :], buf_b[at].reshape(256, 640), preferred_element_type=F32
            )

    for group in range(2):
        for g in wide:
            g.hop(2, group)
        for p in (0, 1, 4, 5)[2 * group : 2 * group + 2]:
            wide_piece(p, 0)
        for p in range(4 * group, 4 * group + 4):
            wide_piece(p, 1)
    for group in range(2):
        for g in wide:
            g.hop(3, group)
        for p in range(4 * group, 4 * group + 4):
            wide_piece(p, 2)
    for j in range(1, 8):
        for g in deep:
            for way in (PLUS, MINUS):
                g.send(way, j)
    for group in range(2):
        for p in range(4 * group, 4 * group + 4):
            wide_piece(p, 3)
        for g in wide:
            g.hop(4, group)
    for p in (0, 1, 4, 5):
        wide_piece(p, 4)

    def deep_hop(hop, group):
        for g in deep:
            g.hop(hop, group)

    deep_hop(1, 0)

    def activate(k, _):
        rows = pl.ds(pl.multiple_of(k * 128, 128), 128)
        gate_at, up_at = (
            jnp.concatenate([v[...].reshape(1, 704), jnp.ones((1, 64), F32)], axis=1) for v in (gs_in, us_in)
        )
        left, right = acc_a[rows, :], acc_b[rows, :]
        tail = right[:, 512:640]
        g = jnp.concatenate([left[:, 0:640], tail], axis=1) * gate_at
        u = jnp.concatenate([left[:, 640:768], right[:, 0:512], pltpu.roll(tail, 64, 1)], axis=1) * up_at
        h = g / (1.0 + jnp.exp(-g)) * u
        lane = lax.broadcasted_iota(jnp.int32, h.shape, 1)
        h = jnp.where(lane < 704, h, 0.0)
        hid[k] = h.T.astype(BF16)
        return 0

    lax.fori_loop(0, 6, activate, 0)

    def half_of(which):
        return jnp.concatenate([hid[which * 3 + k] for k in range(3)], axis=1)

    def exchange(group, at):
        give, got, sem = (give_a, got_a, pair_a) if group == 0 else (give_b, got_b, pair_b)
        return pltpu.make_async_remote_copy(
            src_ref=give.at[at], dst_ref=got.at[at], send_sem=pair_send.at[group], recv_sem=sem.at[at],
            device_id={"tp": peer}, device_id_type=MESH,
        )

    def deep_piece(p, away):
        block, mine = p % 4, p // 4
        sign = 1 if block % 2 == 0 else -1
        group = block // 2
        at = wrap((z, y)[group] + sign * away)
        left = (buf_c, buf_d)[group][at].reshape(128, 768)
        part = jnp.dot(left, half_of(core if mine else other), preferred_element_type=F32)
        if mine:
            (own_a, own_b)[group][at] = part
        else:
            (give_a, give_b)[group][at] = part.astype(BF16)
            exchange(group, at).start()

    def put(group, src, slot, row, owner):
        dst, sem = (all_a.at[slot, core], x_a_sem) if group == 0 else (all_b.at[slot, core, row], x_b_sem)
        return pltpu.make_async_remote_copy(
            src_ref=src, dst_ref=dst, send_sem=x_send.at[group], recv_sem=sem.at[slot, core],
            device_id=(z, y, owner), device_id_type=MESH,
        )

    def relay(group, src, at):
        dst, sem = ((via_a, via_a_sem), (via_b, via_b_sem))[group]
        return pltpu.make_async_remote_copy(
            src_ref=src, dst_ref=dst.at[at], send_sem=x_send.at[group], recv_sem=sem.at[at],
            device_id=(z, y, place(onward, core)), device_id_type=MESH,
        )

    straight_slot = 1 + other
    added_slot = 1 + core

    def combine_one(group, at):
        exchange(group, at).wait_recv()
        if group == 0:
            total = own_a[at] + got_a[at].astype(F32)
            low = total.astype(BF16).reshape(8, 16, 384)
            step = lax.rem(at // 2 - chip + 4, 4)

            @pl.when(at == tp)
            def _():
                all_a[0, core] = low

            @pl.when(at != tp)
            def _():
                sum_a[at] = low

            @pl.when(at == peer)
            def _():
                put(0, sum_a.at[at], 0, 0, at).start()

            @pl.when(step == 2)
            def _():
                relay(0, sum_a.at[at], at).start()

            @pl.when(step == 2 + onward)
            def _():
                put(0, sum_a.at[at], straight_slot, 0, at).start()

            @pl.when(step == 2 - onward)
            def _():
                own_a[at] = total
        else:
            total = own_b[at] + got_b[at].astype(F32)
            sum_b[at] = total.astype(BF16).reshape(8, 16, 384)
            own_b[at] = total
            relay(1, sum_b.at[at, pl.ds(place(2, 0), 2)], at).start()
            for c in (0, 1):
                put(1, sum_b.at[at, place(-onward, c)], straight_slot, at, place(-onward, c)).start()
            put(1, sum_b.at[at, peer], 0, at, peer).start()
            all_b[0, core, at] = sum_b[at, tp]

    def finish_one(group, at):
        if group == 0:
            @pl.when(lax.rem(at // 2 - chip + 4, 4) == 2 - onward)
            def _():
                relay(0, sum_a.at[at], at).wait_recv()
                sum_a[at] = (own_a[at] + via_a[at].reshape(128, 384).astype(F32)).astype(BF16).reshape(8, 16, 384)
                put(0, sum_a.at[at], added_slot, 0, at).start()
        else:
            first = place(onward, 0)
            relay(1, sum_b.at[at, pl.ds(0, 2)], at).wait_recv()
            rows = pl.ds(pl.multiple_of(first * 16, 32), 32)
            total = own_b[at, rows, :] + via_b[at].reshape(32, 384).astype(F32)
            sum_b[at, pl.ds(first, 2)] = total.astype(BF16).reshape(2, 16, 384)
            for c in (0, 1):
                put(1, sum_b.at[at, first + c], added_slot, at, first + c).start()

    def both_sides(act, away):
        for group, me in ((0, z), (1, y)):
            act(group, wrap(me + away))
            if 0 < away < 4:
                act(group, wrap(me - away))

    def combine(away):
        both_sides(combine_one, away)

    def finish(away):
        both_sides(finish_one, away)

    def deep_pieces(which, away):
        for p in which:
            deep_piece(p, away)

    deep_hop(1, 1)
    deep_pieces((0, 2, 4, 6), 0)
    deep_hop(1, 2)
    deep_hop(1, 3)
    combine(0)
    deep_pieces((0, 1, 2, 3), 1)
    deep_hop(2, 0)
    deep_pieces((4, 5), 1)
    deep_hop(2, 1)
    deep_pieces((6, 7), 1)
    combine(1)
    deep_hop(2, 2)
    deep_hop(2, 3)
    finish(0)
    deep_pieces((0, 1, 2, 3), 2)
    deep_hop(3, 0)
    deep_pieces((4, 5, 6, 7), 2)
    deep_hop(3, 1)
    combine(2)
    deep_hop(3, 2)
    deep_hop(3, 3)
    finish(1)
    deep_pieces((0, 1, 2, 3, 4, 5, 6, 7), 3)
    combine(3)
    finish(2)
    deep_hop(4, 0)
    deep_pieces((0, 2, 4, 6), 4)
    combine(4)
    finish(3)
    finish(4)

    for c in range(2):
        for slot in range(3):
            wait_a = pltpu.make_async_copy(all_a.at[slot, c], all_a.at[slot, c], x_a_sem.at[slot, c]).wait
            wait_b = pltpu.make_async_copy(all_b.at[slot, c], all_b.at[slot, c], x_b_sem.at[slot, c]).wait
            if slot:
                wait_a()
                wait_b()
            else:
                pl.when(core != c)(wait_a)
                pl.when(core != c)(wait_b)

    for h, held in ((0, all_a), (1, all_b)):
        for c in range(2):
            total = held[0, c].astype(F32)
            for slot in range(1, 3):
                total += held[slot, c].astype(F32)
            flat[:, h, :, c * 384 : c * 384 + 384] = total
    scale = ds_in[...]
    for k in range(6):
        lanes = slice(k * 128, k * 128 + 128)
        block = flat[:, :, :, lanes].reshape(256, 128)
        out[lanes, :] = (block.T * scale).astype(BF16)

    for g in wide + deep:
        g.drain()
    for group, ref in ((0, give_a), (1, give_b)):
        pltpu.make_async_copy(ref, ref, pair_send.at[group]).wait()
    few = sum_a.at[pl.ds(0, 7)]
    pltpu.make_async_copy(few, few, x_send.at[0]).wait()
    few = sum_b.at[:, pl.ds(0, 7)]
    pltpu.make_async_copy(few, few, x_send.at[1]).wait()


def body(tokens, norm_gain, gate_weight, up_weight, gate_scale, up_scale, down_weight, down_scale):
    vmem = pl.BlockSpec(memory_space=pltpu.VMEM)
    hbm = pl.BlockSpec(memory_space=pl.ANY)
    dma = pltpu.SemaphoreType.DMA
    return pl.pallas_call(
        kernel,
        out_shape=jax.ShapeDtypeStruct((768, 256), BF16),
        in_specs=[hbm] * 8,
        out_specs=vmem,
        scratch_shapes=[
            pltpu.VMEM((768, 2048), BF16),
            pltpu.VMEM((32, 704), F32),
            pltpu.VMEM((32, 704), F32),
            pltpu.VMEM((32, 704), F32),
            pltpu.VMEM((1, 2048), F32),
            pltpu.VMEM((704,), F32),
            pltpu.VMEM((704,), F32),
            pltpu.VMEM((1, 256), F32),
            pltpu.VMEM((512, 512), BF16),
            pltpu.VMEM((2, 8, 768, 256), BF16),
            pltpu.VMEM((8, 8, 32, 768), BF16),
            pltpu.VMEM((8, 8, 32, 640), BF16),
            pltpu.VMEM((8, 8, 16, 768), BF16),
            pltpu.VMEM((8, 8, 16, 768), BF16),
            pltpu.VMEM((768, 768), F32),
            pltpu.VMEM((768, 640), F32),
            pltpu.VMEM((6, 768, 128), BF16),
            pltpu.VMEM((8, 128, 384), F32),
            pltpu.VMEM((8, 128, 384), F32),
            pltpu.VMEM((8, 128, 384), BF16),
            pltpu.VMEM((8, 128, 384), BF16),
            pltpu.VMEM((8, 128, 384), BF16),
            pltpu.VMEM((8, 128, 384), BF16),
            pltpu.VMEM((8, 8, 16, 384), BF16),
            pltpu.VMEM((8, 8, 16, 384), BF16),
            pltpu.VMEM((8, 8, 16, 384), BF16),
            pltpu.VMEM((8, 2, 16, 384), BF16),
            pltpu.VMEM((3, 2, 8, 16, 384), BF16),
            pltpu.VMEM((3, 2, 8, 16, 384), BF16),
            pltpu.VMEM((8, 2, 16, 768), F32),
            dma((8,)),
            dma((4,)),
            dma((4,)),
            dma((4, 2, 4)),
            dma((4, 26)),
            dma((2,)),
            dma((8,)),
            dma((8,)),
            dma((8,)),
            dma((8,)),
            dma((2,)),
            dma((3, 2)),
            dma((3, 2)),
        ],
        compiler_params=pltpu.CompilerParams(
            collective_id=0, has_side_effects=True, vmem_limit_bytes=56 * 1024 * 1024
        ),
    )(
        tokens, norm_gain.reshape(1, 2048), gate_weight, up_weight, gate_scale, up_scale,
        down_weight.T, down_scale.reshape(1, 256),
    )


def solution(mesh):
    split = Mesh(mesh.devices.reshape(8, 8, mesh.shape["tp"]), ("fs_0", "fs_1", "tp"))
    placed = (P(FS, None), P(), P(FS, "tp"), P(FS, "tp"), P("tp"), P("tp"), P("tp", FS), P("tp"))
    return jax.shard_map(body, mesh=split, in_specs=placed, out_specs=P(FS, "tp"), check_vma=False)
```

```python
import jax
import jax.numpy as jnp
from jax import lax
from jax.experimental import pallas as pl
from jax.experimental.pallas import tpu as pltpu
from jax.sharding import Mesh
from jax.sharding import PartitionSpec as P

FS = ("fs_0", "fs_1")
MESH = pl.DeviceIdType.MESH
F32, BF16 = jnp.float32, jnp.bfloat16
OFF = (0, 1, -1, 2, -2, 3, -3, 4)
PLUS, MINUS = 0, 1
WIDE, DEEP = (2, 4, 4, 4), (2, 2, 2, 8)


def wrap(i):
    return lax.rem(i + 16, 8)


class Gather:
    def __init__(self, buf, major, minor, along_major, along_minor, sems, sizes):
        self.buf, self.major, self.minor, self.sizes = buf, major, minor, sizes
        self.along_major, self.along_minor = along_major, along_minor
        self.send1, self.send2, self.recv1, self.recv2 = sems

    def first(self, way, step, source):
        at = self.buf.at[self.major, wrap(self.minor + source)]
        return pltpu.make_async_remote_copy(
            src_ref=at, dst_ref=at, send_sem=self.send1, recv_sem=self.recv1.at[way, step - 1],
            device_id=self.along_minor[way], device_id_type=MESH,
        )

    def second(self, way, hop, j, source):
        at = self.buf.at[wrap(self.major + source), wrap(self.minor + OFF[j])]
        if hop == 4:
            at = at.at[self.half(way)]
        return pltpu.make_async_remote_copy(
            src_ref=at, dst_ref=at, send_sem=self.send2, recv_sem=self.recv2.at[self.number(way, hop, j // self.sizes[hop - 1])],
            device_id=self.along_major[way], device_id_type=MESH,
        )

    def start_first(self):
        self.first(PLUS, 1, 0).start()
        self.first(MINUS, 1, 0).start()

    def half(self, way):
        length = self.buf.shape[2]
        return pl.ds(0, length // 2) if way == PLUS else pl.ds(length // 2, length - length // 2)

    def send(self, way, j):
        self.second(way, 1, j, 0).start()

    def number(self, way, hop, group):
        counts = [8 // size for size in self.sizes]
        return 2 * sum(counts[: hop - 1]) + way * counts[hop - 1] + group

    def arrive(self, way, hop, group):
        size = self.sizes[hop - 1]
        here = self.buf.at[0, pl.ds(0, size)]
        if hop == 4:
            here = self.buf.at[0, pl.ds(0, size), self.half(way)]
        pltpu.make_async_copy(here, here, self.recv2.at[self.number(way, hop, group)]).wait()

    def line(self, step):
        self.first(PLUS, step, -step).wait_recv()
        if step < 4:
            self.first(PLUS, step + 1, -step).start()
            self.first(MINUS, step, step).wait_recv()
        if step < 3:
            self.first(MINUS, step + 1, step).start()

    def hop(self, hop, group):
        size = self.sizes[hop - 1]
        for way, side in ((PLUS, -1), (MINUS, 1)):
            self.arrive(way, hop, group)
            if hop < 4:
                for j in range(group * size, group * size + size):
                    self.second(way, hop + 1, j, side * hop).start()

    def drain(self):
        one = self.buf.at[0, pl.ds(0, 7)]
        many = self.buf.at[pl.ds(0, 7)]
        for ref, sem in ((one, self.send1), (many, self.send2)):
            pltpu.make_async_copy(ref, ref, sem).wait()


def kernel(
    tokens, gain, gate_w, up_w, gate_s, up_s, down_w, down_s, out,
    tok, gw_in, uw_in, dw_in, gain_in, gs_in, us_in, ds_in, perm, x_all, buf_a, buf_b, buf_c, buf_d, acc_a, acc_b, hid,
    own_a, own_b, give_a, give_b, got_a, got_b, sum_a, sum_b, via_a, via_b, all_a, all_b, flat,
    in_sem, send1, send2, recv1, recv2, pair_send, pair_a, pair_b, via_a_sem, via_b_sem, x_send, x_a_sem, x_b_sem,
):
    z, y, tp = lax.axis_index("fs_0"), lax.axis_index("fs_1"), lax.axis_index("tp")
    core = lax.rem(tp, 2)
    other = 1 - core
    peer = tp + 1 - 2 * core
    chip = tp // 2
    onward = 1 - 2 * core

    def place(step, c):
        return 2 * lax.rem(chip + step + 8, 4) + c

    along_z = [(wrap(z + side), y, tp) for side in (1, -1)]
    along_y = [(z, wrap(y + side), tp) for side in (1, -1)]
    barrier = pltpu.get_barrier_semaphore()
    near = along_z + along_y + [(z, y, peer)] + [(z, y, place(step, c)) for step in (1, 3) for c in (0, 1)]
    for device in near:
        pl.semaphore_signal(barrier, inc=1, device_id=device, device_id_type=MESH)

    inputs = (
        (gate_w, gw_in), (up_w, uw_in), (down_w, dw_in), (tokens, tok), (gain, gain_in), (gate_s, gs_in), (up_s, us_in), (down_s, ds_in),
    )
    fetches = [
        pltpu.make_async_copy(src, dst, in_sem.at[k])
        for k, (src, dst) in enumerate(inputs)
    ]
    for fetch in fetches:
        fetch.start()

    major = z + core * (y - z)
    minor = y + core * (z - y)

    def either(first, second):
        return [tuple(f + core * (s - f) for f, s in zip(one, two)) for one, two in zip(first, second)]

    along_major, along_minor = either(along_z, along_y), either(along_y, along_z)

    def sems(k):
        return send1.at[k], send2.at[k], recv1.at[k], recv2.at[k]

    ga = Gather(buf_a, major, minor, along_major, along_minor, sems(0), WIDE)
    gb = Gather(buf_b, minor, major, along_minor, along_major, sems(1), WIDE)
    gc = Gather(buf_c, z, y, along_z, along_y, sems(2), DEEP)
    gd = Gather(buf_d, y, z, along_y, along_z, sems(3), DEEP)
    wide, deep = (ga, gb), (gc, gd)

    fetches[0].wait()
    fetches[1].wait()
    gw, uw = gw_in[...].astype(BF16), uw_in[...].astype(BF16)
    buf_a[major, minor, :, 0:640] = gw[:, 0:640]
    buf_a[major, minor, :, 640:768] = uw[:, 0:128]
    buf_b[minor, major, :, 0:512] = uw[:, 128:640]
    buf_b[minor, major, :, 512:640] = jnp.concatenate([gw[:, 640:], uw[:, 640:]], axis=1)
    pl.semaphore_wait(barrier, len(near))
    for g in wide:
        g.start_first()
    for g in wide:
        for way in (PLUS, MINUS):
            g.send(way, 0)
    fetches[2].wait()
    for top, place_of in ((0, buf_c.at[z, y]), (16, buf_d.at[y, z])):
        upper, lower = dw_in[top : top + 8, :], dw_in[top + 8 : top + 16, :]
        for k in range(5):
            place_of[2 * k] = upper[:, k * 128 : k * 128 + 128].astype(BF16)
            place_of[2 * k + 1] = lower[:, k * 128 : k * 128 + 128].astype(BF16)
        place_of[10] = jnp.concatenate([upper[:, 640:], lower[:, 640:]], axis=1).astype(BF16)
    for g in deep:
        g.start_first()
    for g in deep:
        for way in (PLUS, MINUS):
            g.send(way, 0)

    for fetch in fetches[3:]:
        fetch.wait()

    def normalize(k, _):
        rows = pl.ds(pl.multiple_of(k * 64, 64), 64)
        squares = jnp.zeros((64, 128), F32)
        for t in range(16):
            v = tok[rows, t * 128 : t * 128 + 128].astype(F32)
            squares += v * v
        factor = lax.rsqrt(jnp.sum(squares, axis=-1, keepdims=True) * (1 / 2048) + 1e-06)
        for t in range(16):
            v = tok[rows, t * 128 : t * 128 + 128].astype(F32) * factor * gain_in[:, t * 128 : t * 128 + 128]
            x_all[0, t // 2, rows, t % 2 * 128 : t % 2 * 128 + 128] = v.astype(BF16)
        return 0

    lax.fori_loop(0, 5, normalize, 0)

    k, n = (lax.broadcasted_iota(jnp.int32, (512, 512), d) for d in (0, 1))
    chosen = (k // 128 == n % 128 // 32) & (k % 128 // 32 == n // 128) & (k % 32 == n % 32)
    perm[...] = chosen.astype(F32).astype(BF16)

    def permute(group):
        zh, yh = group // 2, group % 2

        def some(k, _):
            rows = pl.ds(pl.multiple_of(k * 256, 256), 256)
            source = jnp.concatenate([x_all[0, zh * 4 + zl, rows, yh * 128 : yh * 128 + 128] for zl in range(4)], axis=1)
            moved = jnp.dot(source, perm[...], preferred_element_type=F32).astype(BF16)
            for yq in range(4):
                x_all[1, yh * 4 + yq, rows, zh * 128 : zh * 128 + 128] = moved[:, yq * 128 : yq * 128 + 128]
            return 0

        lax.fori_loop(0, 3, some, 0)

    for step in range(1, 5):
        for g in wide:
            g.line(step)
            for j in (2 * step - 1, 2 * step):
                for way in (PLUS, MINUS):
                    if j < 8:
                        g.send(way, j)
        for g in deep:
            g.line(step)
        if step < 4:
            lax.fori_loop((5, 8, 10)[step - 1], (8, 10, 12)[step - 1], normalize, 0)
        if step > 1:
            for g in wide:
                g.hop(1, step - 2)
    permute(0)
    permute(1)
    for g in wide:
        g.hop(1, 3)
    permute(2)
    permute(3)
    acc_a[...] = jnp.zeros_like(acc_a)
    acc_b[...] = jnp.zeros_like(acc_b)

    def wide_piece(p, away):
        block, half = p // 2, p % 2
        sign = 1 if block % 2 == 0 else -1
        rows = slice(half * 384, half * 384 + 384)
        if block < 2:
            at = wrap(major + sign * away)
            acc_a[rows, :] += jnp.dot(
                x_all[core, at, rows, :], buf_a[at].reshape(256, 768), preferred_element_type=F32
            )
        else:
            at = wrap(minor + sign * away)
            acc_b[rows, :] += jnp.dot(
                x_all[other, at, rows, :], buf_b[at].reshape(256, 640), preferred_element_type=F32
            )

    for group in range(2):
        for g in wide:
            g.hop(2, group)
        for p in (0, 1, 4, 5)[2 * group : 2 * group + 2]:
            wide_piece(p, 0)
        for p in range(4 * group, 4 * group + 4):
            wide_piece(p, 1)
    for group in range(2):
        for g in wide:
            g.hop(3, group)
        for p in range(4 * group, 4 * group + 4):
            wide_piece(p, 2)
    for j in range(1, 8):
        for g in deep:
            for way in (PLUS, MINUS):
                g.send(way, j)
    for group in range(2):
        for p in range(4 * group, 4 * group + 4):
            wide_piece(p, 3)
        for g in wide:
            g.hop(4, group)
    for p in (0, 1, 4, 5):
        wide_piece(p, 4)

    def deep_hop(hop, group):
        for g in deep:
            g.hop(hop, group)

    deep_hop(1, 0)

    def activate(k, _):
        rows = pl.ds(pl.multiple_of(k * 128, 128), 128)
        gate_at, up_at = (
            jnp.concatenate([v[...].reshape(1, 704), jnp.ones((1, 64), F32)], axis=1) for v in (gs_in, us_in)
        )
        left, right = acc_a[rows, :], acc_b[rows, :]
        tail = right[:, 512:640]
        g = jnp.concatenate([left[:, 0:640], tail], axis=1) * gate_at
        u = jnp.concatenate([left[:, 640:768], right[:, 0:512], pltpu.roll(tail, 64, 1)], axis=1) * up_at
        h = g / (1.0 + jnp.exp(-g)) * u
        lane = lax.broadcasted_iota(jnp.int32, h.shape, 1)
        h = jnp.where(lane < 704, h, 0.0)
        hid[k] = h.T.astype(BF16)
        return 0

    lax.fori_loop(0, 6, activate, 0)

    def half_of(which):
        return jnp.concatenate([hid[which * 3 + k] for k in range(3)], axis=1)

    def exchange(group, at):
        give, got, sem = (give_a, got_a, pair_a) if group == 0 else (give_b, got_b, pair_b)
        return pltpu.make_async_remote_copy(
            src_ref=give.at[at], dst_ref=got.at[at], send_sem=pair_send.at[group], recv_sem=sem.at[at],
            device_id={"tp": peer}, device_id_type=MESH,
        )

    def deep_piece(p, away):
        block, mine = p % 4, p // 4
        sign = 1 if block % 2 == 0 else -1
        group = block // 2
        at = wrap((z, y)[group] + sign * away)
        tiles = (buf_c, buf_d)[group]
        upper = tiles[at, :, 10].astype(F32)
        lower = pltpu.roll(upper.reshape(64, 128), 64, 1).reshape(8, 8, 128)
        last = jnp.stack([upper, lower], axis=1).reshape(128, 128).astype(BF16)
        left = jnp.concatenate([tiles[at, :, 2 * k : 2 * k + 2].reshape(128, 128) for k in range(5)] + [last], axis=1)
        part = jnp.dot(left, half_of(core if mine else other), preferred_element_type=F32)
        if mine:
            (own_a, own_b)[group][at] = part
        else:
            (give_a, give_b)[group][at] = part.astype(BF16)
            exchange(group, at).start()

    def put(group, src, slot, row, owner):
        dst, sem = (all_a.at[slot, core], x_a_sem) if group == 0 else (all_b.at[slot, core, row], x_b_sem)
        return pltpu.make_async_remote_copy(
            src_ref=src, dst_ref=dst, send_sem=x_send.at[group], recv_sem=sem.at[slot, core],
            device_id=(z, y, owner), device_id_type=MESH,
        )

    def relay(group, src, at):
        dst, sem = ((via_a, via_a_sem), (via_b, via_b_sem))[group]
        return pltpu.make_async_remote_copy(
            src_ref=src, dst_ref=dst.at[at], send_sem=x_send.at[group], recv_sem=sem.at[at],
            device_id=(z, y, place(onward, core)), device_id_type=MESH,
        )

    straight_slot = 1 + other
    added_slot = 1 + core

    def combine_one(group, at):
        exchange(group, at).wait_recv()
        if group == 0:
            total = own_a[at] + got_a[at].astype(F32)
            low = total.astype(BF16).reshape(8, 16, 384)
            step = lax.rem(at // 2 - chip + 4, 4)

            @pl.when(at == tp)
            def _():
                all_a[0, core] = low

            @pl.when(at != tp)
            def _():
                sum_a[at] = low

            @pl.when(at == peer)
            def _():
                put(0, sum_a.at[at], 0, 0, at).start()

            @pl.when(step == 2)
            def _():
                relay(0, sum_a.at[at], at).start()

            @pl.when(step == 2 + onward)
            def _():
                put(0, sum_a.at[at], straight_slot, 0, at).start()

            @pl.when(step == 2 - onward)
            def _():
                own_a[at] = total
        else:
            total = own_b[at] + got_b[at].astype(F32)
            sum_b[at] = total.astype(BF16).reshape(8, 16, 384)
            own_b[at] = total
            relay(1, sum_b.at[at, pl.ds(place(2, 0), 2)], at).start()
            for c in (0, 1):
                put(1, sum_b.at[at, place(-onward, c)], straight_slot, at, place(-onward, c)).start()
            put(1, sum_b.at[at, peer], 0, at, peer).start()
            all_b[0, core, at] = sum_b[at, tp]

    def finish_one(group, at):
        if group == 0:
            @pl.when(lax.rem(at // 2 - chip + 4, 4) == 2 - onward)
            def _():
                relay(0, sum_a.at[at], at).wait_recv()
                sum_a[at] = (own_a[at] + via_a[at].reshape(128, 384).astype(F32)).astype(BF16).reshape(8, 16, 384)
                put(0, sum_a.at[at], added_slot, 0, at).start()
        else:
            first = place(onward, 0)
            relay(1, sum_b.at[at, pl.ds(0, 2)], at).wait_recv()
            rows = pl.ds(pl.multiple_of(first * 16, 32), 32)
            total = own_b[at, rows, :] + via_b[at].reshape(32, 384).astype(F32)
            sum_b[at, pl.ds(first, 2)] = total.astype(BF16).reshape(2, 16, 384)
            for c in (0, 1):
                put(1, sum_b.at[at, first + c], added_slot, at, first + c).start()

    def both_sides(act, away):
        for group, me in ((0, z), (1, y)):
            act(group, wrap(me + away))
            if 0 < away < 4:
                act(group, wrap(me - away))

    def combine(away):
        both_sides(combine_one, away)

    def finish(away):
        both_sides(finish_one, away)

    def deep_pieces(which, away):
        for p in which:
            deep_piece(p, away)

    deep_hop(1, 1)
    deep_pieces((0, 2, 4, 6), 0)
    deep_hop(1, 2)
    deep_hop(1, 3)
    combine(0)
    deep_pieces((0, 1, 2, 3), 1)
    deep_hop(2, 0)
    deep_pieces((4, 5), 1)
    deep_hop(2, 1)
    deep_pieces((6, 7), 1)
    combine(1)
    deep_hop(2, 2)
    deep_hop(2, 3)
    finish(0)
    deep_pieces((0, 1, 2, 3), 2)
    deep_hop(3, 0)
    deep_pieces((4, 5, 6, 7), 2)
    deep_hop(3, 1)
    combine(2)
    deep_hop(3, 2)
    deep_hop(3, 3)
    finish(1)
    deep_pieces((0, 1, 2, 3, 4, 5, 6, 7), 3)
    combine(3)
    finish(2)
    deep_hop(4, 0)
    deep_pieces((0, 2, 4, 6), 4)
    combine(4)
    finish(3)
    finish(4)

    for c in range(2):
        for slot in range(3):
            wait_a = pltpu.make_async_copy(all_a.at[slot, c], all_a.at[slot, c], x_a_sem.at[slot, c]).wait
            wait_b = pltpu.make_async_copy(all_b.at[slot, c], all_b.at[slot, c], x_b_sem.at[slot, c]).wait
            if slot:
                wait_a()
                wait_b()
            else:
                pl.when(core != c)(wait_a)
                pl.when(core != c)(wait_b)

    for h, held in ((0, all_a), (1, all_b)):
        for c in range(2):
            total = held[0, c].astype(F32)
            for slot in range(1, 3):
                total += held[slot, c].astype(F32)
            flat[:, h, :, c * 384 : c * 384 + 384] = total
    scale = ds_in[...]
    for k in range(6):
        lanes = slice(k * 128, k * 128 + 128)
        block = flat[:, :, :, lanes].reshape(256, 128)
        out[lanes, :] = (block.T * scale).astype(BF16)

    for g in wide + deep:
        g.drain()
    for group, ref in ((0, give_a), (1, give_b)):
        pltpu.make_async_copy(ref, ref, pair_send.at[group]).wait()
    few = sum_a.at[pl.ds(0, 7)]
    pltpu.make_async_copy(few, few, x_send.at[0]).wait()
    few = sum_b.at[:, pl.ds(0, 7)]
    pltpu.make_async_copy(few, few, x_send.at[1]).wait()


def body(tokens, norm_gain, gate_weight, up_weight, gate_scale, up_scale, down_weight, down_scale):
    vmem = pl.BlockSpec(memory_space=pltpu.VMEM)
    hbm = pl.BlockSpec(memory_space=pl.ANY)
    dma = pltpu.SemaphoreType.DMA
    return pl.pallas_call(
        kernel,
        out_shape=jax.ShapeDtypeStruct((768, 256), BF16),
        in_specs=[hbm] * 8,
        out_specs=vmem,
        scratch_shapes=[
            pltpu.VMEM((768, 2048), BF16),
            pltpu.VMEM((32, 704), F32),
            pltpu.VMEM((32, 704), F32),
            pltpu.VMEM((32, 704), F32),
            pltpu.VMEM((1, 2048), F32),
            pltpu.VMEM((704,), F32),
            pltpu.VMEM((704,), F32),
            pltpu.VMEM((1, 256), F32),
            pltpu.VMEM((512, 512), BF16),
            pltpu.VMEM((2, 8, 768, 256), BF16),
            pltpu.VMEM((8, 8, 32, 768), BF16),
            pltpu.VMEM((8, 8, 32, 640), BF16),
            pltpu.VMEM((8, 8, 11, 8, 128), BF16),
            pltpu.VMEM((8, 8, 11, 8, 128), BF16),
            pltpu.VMEM((768, 768), F32),
            pltpu.VMEM((768, 640), F32),
            pltpu.VMEM((6, 768, 128), BF16),
            pltpu.VMEM((8, 128, 384), F32),
            pltpu.VMEM((8, 128, 384), F32),
            pltpu.VMEM((8, 128, 384), BF16),
            pltpu.VMEM((8, 128, 384), BF16),
            pltpu.VMEM((8, 128, 384), BF16),
            pltpu.VMEM((8, 128, 384), BF16),
            pltpu.VMEM((8, 8, 16, 384), BF16),
            pltpu.VMEM((8, 8, 16, 384), BF16),
            pltpu.VMEM((8, 8, 16, 384), BF16),
            pltpu.VMEM((8, 2, 16, 384), BF16),
            pltpu.VMEM((3, 2, 8, 16, 384), BF16),
            pltpu.VMEM((3, 2, 8, 16, 384), BF16),
            pltpu.VMEM((8, 2, 16, 768), F32),
            dma((8,)),
            dma((4,)),
            dma((4,)),
            dma((4, 2, 4)),
            dma((4, 26)),
            dma((2,)),
            dma((8,)),
            dma((8,)),
            dma((8,)),
            dma((8,)),
            dma((2,)),
            dma((3, 2)),
            dma((3, 2)),
        ],
        compiler_params=pltpu.CompilerParams(
            collective_id=0, has_side_effects=True, vmem_limit_bytes=56 * 1024 * 1024
        ),
    )(
        tokens, norm_gain.reshape(1, 2048), gate_weight, up_weight, gate_scale, up_scale,
        down_weight.T, down_scale.reshape(1, 256),
    )


def solution(mesh):
    split = Mesh(mesh.devices.reshape(8, 8, mesh.shape["tp"]), ("fs_0", "fs_1", "tp"))
    placed = (P(FS, None), P(), P(FS, "tp"), P(FS, "tp"), P("tp"), P("tp"), P("tp", FS), P("tp"))
    return jax.shard_map(body, mesh=split, in_specs=placed, out_specs=P(FS, "tp"), check_vma=False)
```

```python
import jax
import jax.numpy as jnp
from jax import lax
from jax.experimental import pallas as pl
from jax.experimental.pallas import tpu as pltpu
from jax.sharding import Mesh
from jax.sharding import PartitionSpec as P

FS = ("fs_0", "fs_1")
MESH = pl.DeviceIdType.MESH
F32, BF16 = jnp.float32, jnp.bfloat16
OFF = (0, 1, -1, 2, -2, 3, -3, 4)
PLUS, MINUS = 0, 1
WIDE, DEEP = (2, 4, 4, 8), (2, 2, 2, 8)


def wrap(i):
    return lax.rem(i + 16, 8)


class Gather:
    def __init__(self, buf, major, minor, along_major, along_minor, sems, sizes):
        self.buf, self.major, self.minor, self.sizes = buf, major, minor, sizes
        self.along_major, self.along_minor = along_major, along_minor
        self.send1, self.send2, self.recv1, self.recv2 = sems

    def first(self, way, step, source):
        at = self.buf.at[self.major, wrap(self.minor + source)]
        return pltpu.make_async_remote_copy(
            src_ref=at, dst_ref=at, send_sem=self.send1, recv_sem=self.recv1.at[way, step - 1],
            device_id=self.along_minor[way], device_id_type=MESH,
        )

    def second(self, way, hop, j, source):
        at = self.buf.at[wrap(self.major + source), wrap(self.minor + OFF[j])]
        if hop == 4:
            at = at.at[self.half(way)]
        return pltpu.make_async_remote_copy(
            src_ref=at, dst_ref=at, send_sem=self.send2, recv_sem=self.recv2.at[self.number(way, hop, j // self.sizes[hop - 1])],
            device_id=self.along_major[way], device_id_type=MESH,
        )

    def start_first(self):
        self.first(PLUS, 1, 0).start()
        self.first(MINUS, 1, 0).start()

    def half(self, way):
        length = self.buf.shape[2]
        return pl.ds(0, length // 2) if way == PLUS else pl.ds(length // 2, length - length // 2)

    def send(self, way, j):
        self.second(way, 1, j, 0).start()

    def number(self, way, hop, group):
        counts = [8 // size for size in self.sizes]
        return 2 * sum(counts[: hop - 1]) + way * counts[hop - 1] + group

    def arrive(self, way, hop, group):
        size = self.sizes[hop - 1]
        here = self.buf.at[0, pl.ds(0, size)]
        if hop == 4:
            here = self.buf.at[0, pl.ds(0, size), self.half(way)]
        pltpu.make_async_copy(here, here, self.recv2.at[self.number(way, hop, group)]).wait()

    def line(self, step):
        self.first(PLUS, step, -step).wait_recv()
        if step < 4:
            self.first(PLUS, step + 1, -step).start()
            self.first(MINUS, step, step).wait_recv()
        if step < 3:
            self.first(MINUS, step + 1, step).start()

    def hop(self, hop, group):
        size = self.sizes[hop - 1]
        for way, side in ((PLUS, -1), (MINUS, 1)):
            self.arrive(way, hop, group)
            if hop < 4:
                for j in range(group * size, group * size + size):
                    self.second(way, hop + 1, j, side * hop).start()

    def drain(self):
        one = self.buf.at[0, pl.ds(0, 7)]
        many = self.buf.at[pl.ds(0, 7)]
        for ref, sem in ((one, self.send1), (many, self.send2)):
            pltpu.make_async_copy(ref, ref, sem).wait()


def kernel(
    tokens, gain, gate_w, up_w, gate_s, up_s, down_w, down_s, out,
    tok, gw_in, uw_in, dw_in, gain_in, gs_in, us_in, ds_in, perm, x_all, buf_a, buf_b, buf_c, buf_d, acc_a, acc_b, hid,
    own_a, own_b, give_a, give_b, got_a, got_b, sum_a, sum_b, via_a, via_b, all_a, all_b, flat,
    in_sem, send1, send2, recv1, recv2, pair_send, pair_recv, via_a_sem, via_b_sem, x_send, x_a_sem, x_b_sem,
):
    z, y, tp = lax.axis_index("fs_0"), lax.axis_index("fs_1"), lax.axis_index("tp")
    core = lax.rem(tp, 2)
    other = 1 - core
    peer = tp + 1 - 2 * core
    chip = tp // 2
    onward = 1 - 2 * core

    def place(step, c):
        return 2 * lax.rem(chip + step + 8, 4) + c

    along_z = [(wrap(z + side), y, tp) for side in (1, -1)]
    along_y = [(z, wrap(y + side), tp) for side in (1, -1)]
    barrier = pltpu.get_barrier_semaphore()
    near = along_z + along_y + [(z, y, peer)] + [(z, y, place(step, c)) for step in (1, 3) for c in (0, 1)]
    for device in near:
        pl.semaphore_signal(barrier, inc=1, device_id=device, device_id_type=MESH)

    inputs = (
        (gate_w, gw_in), (up_w, uw_in), (down_w, dw_in), (tokens, tok), (gain, gain_in), (gate_s, gs_in), (up_s, us_in), (down_s, ds_in),
    )
    fetches = [
        pltpu.make_async_copy(src, dst, in_sem.at[k])
        for k, (src, dst) in enumerate(inputs)
    ]
    for fetch in fetches:
        fetch.start()

    major = z + core * (y - z)
    minor = y + core * (z - y)

    def either(first, second):
        return [tuple(f + core * (s - f) for f, s in zip(one, two)) for one, two in zip(first, second)]

    along_major, along_minor = either(along_z, along_y), either(along_y, along_z)

    def sems(k):
        return send1.at[k], send2.at[k], recv1.at[k], recv2.at[k]

    ga = Gather(buf_a, major, minor, along_major, along_minor, sems(0), WIDE)
    gb = Gather(buf_b, minor, major, along_minor, along_major, sems(1), WIDE)
    gc = Gather(buf_c, z, y, along_z, along_y, sems(2), DEEP)
    gd = Gather(buf_d, y, z, along_y, along_z, sems(3), DEEP)
    wide, deep = (ga, gb), (gc, gd)

    fetches[0].wait()
    fetches[1].wait()
    gw, uw = gw_in[...].astype(BF16), uw_in[...].astype(BF16)
    buf_a[major, minor, :, 0:640] = gw[:, 0:640]
    buf_a[major, minor, :, 640:768] = uw[:, 0:128]
    buf_b[minor, major, :, 0:512] = uw[:, 128:640]
    buf_b[minor, major, :, 512:640] = jnp.concatenate([gw[:, 640:], uw[:, 640:]], axis=1)
    pl.semaphore_wait(barrier, len(near))
    for g in wide:
        g.start_first()
    for g in wide:
        for way in (PLUS, MINUS):
            g.send(way, 0)
    fetches[2].wait()
    for top, place_of in ((0, buf_c.at[z, y]), (16, buf_d.at[y, z])):
        upper, lower = dw_in[top : top + 8, :], dw_in[top + 8 : top + 16, :]
        for k in range(5):
            place_of[2 * k] = upper[:, k * 128 : k * 128 + 128].astype(BF16)
            place_of[2 * k + 1] = lower[:, k * 128 : k * 128 + 128].astype(BF16)
        place_of[10] = jnp.concatenate([upper[:, 640:], lower[:, 640:]], axis=1).astype(BF16)
    for g in deep:
        g.start_first()
    for g in deep:
        for way in (PLUS, MINUS):
            g.send(way, 0)

    for fetch in fetches[3:]:
        fetch.wait()

    def normalize(k, _):
        rows = pl.ds(pl.multiple_of(k * 64, 64), 64)
        squares = jnp.zeros((64, 128), F32)
        for t in range(16):
            v = tok[rows, t * 128 : t * 128 + 128].astype(F32)
            squares += v * v
        factor = lax.rsqrt(jnp.sum(squares, axis=-1, keepdims=True) * (1 / 2048) + 1e-06)
        for t in range(16):
            v = tok[rows, t * 128 : t * 128 + 128].astype(F32) * factor * gain_in[:, t * 128 : t * 128 + 128]
            x_all[0, t // 2, rows, t % 2 * 128 : t % 2 * 128 + 128] = v.astype(BF16)
        return 0

    lax.fori_loop(0, 5, normalize, 0)

    k, n = (lax.broadcasted_iota(jnp.int32, (512, 512), d) for d in (0, 1))
    chosen = (k // 128 == n % 128 // 32) & (k % 128 // 32 == n // 128) & (k % 32 == n % 32)
    perm[...] = chosen.astype(F32).astype(BF16)

    def permute(group):
        zh, yh = group // 2, group % 2

        def some(k, _):
            rows = pl.ds(pl.multiple_of(k * 256, 256), 256)
            source = jnp.concatenate([x_all[0, zh * 4 + zl, rows, yh * 128 : yh * 128 + 128] for zl in range(4)], axis=1)
            moved = jnp.dot(source, perm[...], preferred_element_type=F32).astype(BF16)
            for yq in range(4):
                x_all[1, yh * 4 + yq, rows, zh * 128 : zh * 128 + 128] = moved[:, yq * 128 : yq * 128 + 128]
            return 0

        lax.fori_loop(0, 3, some, 0)

    for step in range(1, 5):
        for g in wide:
            g.line(step)
            for j in (2 * step - 1, 2 * step):
                for way in (PLUS, MINUS):
                    if j < 8:
                        g.send(way, j)
        for g in deep:
            g.line(step)
        if step < 4:
            lax.fori_loop((5, 8, 10)[step - 1], (8, 10, 12)[step - 1], normalize, 0)
        if step > 1:
            for g in wide:
                g.hop(1, step - 2)
    permute(0)
    permute(1)
    for g in wide:
        g.hop(1, 3)
    permute(2)
    permute(3)
    acc_a[...] = jnp.zeros_like(acc_a)
    acc_b[...] = jnp.zeros_like(acc_b)

    def wide_piece(p, away):
        block, half = p // 2, p % 2
        sign = 1 if block % 2 == 0 else -1
        rows = slice(half * 384, half * 384 + 384)
        if block < 2:
            at = wrap(major + sign * away)
            acc_a[rows, :] += jnp.dot(
                x_all[core, at, rows, :], buf_a[at].reshape(256, 768), preferred_element_type=F32
            )
        else:
            at = wrap(minor + sign * away)
            acc_b[rows, :] += jnp.dot(
                x_all[other, at, rows, :], buf_b[at].reshape(256, 640), preferred_element_type=F32
            )

    for group in range(2):
        for g in wide:
            g.hop(2, group)
        for p in (0, 1, 4, 5)[2 * group : 2 * group + 2]:
            wide_piece(p, 0)
        for p in range(4 * group, 4 * group + 4):
            wide_piece(p, 1)
    for group in range(2):
        for g in wide:
            g.hop(3, group)
        for p in range(4 * group, 4 * group + 4):
            wide_piece(p, 2)
    for j in range(1, 8):
        for g in deep:
            for way in (PLUS, MINUS):
                g.send(way, j)
    for group in range(2):
        for p in range(4 * group, 4 * group + 4):
            wide_piece(p, 3)
    for g in wide:
        g.hop(4, 0)
    for p in (0, 1, 4, 5):
        wide_piece(p, 4)

    def deep_hop(hop, group):
        for g in deep:
            g.hop(hop, group)

    deep_hop(1, 0)

    def activate(k, _):
        rows = pl.ds(pl.multiple_of(k * 128, 128), 128)
        gate_at, up_at = (
            jnp.concatenate([v[...].reshape(1, 704), jnp.ones((1, 64), F32)], axis=1) for v in (gs_in, us_in)
        )
        left, right = acc_a[rows, :], acc_b[rows, :]
        tail = right[:, 512:640]
        g = jnp.concatenate([left[:, 0:640], tail], axis=1) * gate_at
        u = jnp.concatenate([left[:, 640:768], right[:, 0:512], pltpu.roll(tail, 64, 1)], axis=1) * up_at
        h = g / (1.0 + jnp.exp(-g)) * u
        lane = lax.broadcasted_iota(jnp.int32, h.shape, 1)
        h = jnp.where(lane < 704, h, 0.0)
        hid[k] = h.T.astype(BF16)
        return 0

    lax.fori_loop(0, 6, activate, 0, unroll=2)

    def half_of(which):
        return jnp.concatenate([hid[which * 3 + k] for k in range(3)], axis=1)

    def exchange(group, at, away):
        give, got = (give_a, got_a) if group == 0 else (give_b, got_b)
        return pltpu.make_async_remote_copy(
            src_ref=give.at[at], dst_ref=got.at[at], send_sem=pair_send.at[group], recv_sem=pair_recv.at[away],
            device_id={"tp": peer}, device_id_type=MESH,
        )

    def deep_piece(p, away):
        block, mine = p % 4, p // 4
        sign = 1 if block % 2 == 0 else -1
        group = block // 2
        at = wrap((z, y)[group] + sign * away)
        tiles = (buf_c, buf_d)[group]
        upper = tiles[at, :, 10].astype(F32)
        lower = pltpu.roll(upper.reshape(64, 128), 64, 1).reshape(8, 8, 128)
        last = jnp.stack([upper, lower], axis=1).reshape(128, 128).astype(BF16)
        left = jnp.concatenate([tiles[at, :, 2 * k : 2 * k + 2].reshape(128, 128) for k in range(5)] + [last], axis=1)
        part = jnp.dot(left, half_of(core if mine else other), preferred_element_type=F32)
        if mine:
            (own_a, own_b)[group][at] = part
        else:
            (give_a, give_b)[group][at] = part.astype(BF16)
            exchange(group, at, away).start()

    def put(group, src, slot, row, owner):
        dst, sem = (all_a.at[slot, core], x_a_sem) if group == 0 else (all_b.at[slot, core, row], x_b_sem)
        return pltpu.make_async_remote_copy(
            src_ref=src, dst_ref=dst, send_sem=x_send.at[group], recv_sem=sem.at[slot, core],
            device_id=(z, y, owner), device_id_type=MESH,
        )

    def relay(group, src, at):
        dst, sem = ((via_a, via_a_sem), (via_b, via_b_sem))[group]
        return pltpu.make_async_remote_copy(
            src_ref=src, dst_ref=dst.at[at], send_sem=x_send.at[group], recv_sem=sem.at[at],
            device_id=(z, y, place(onward, core)), device_id_type=MESH,
        )

    straight_slot = 1 + other
    added_slot = 1 + core

    def combine_one(group, at):
        if group == 0:
            total = own_a[at] + got_a[at].astype(F32)
            low = total.astype(BF16).reshape(8, 16, 384)
            step = lax.rem(at // 2 - chip + 4, 4)

            @pl.when(at == tp)
            def _():
                all_a[0, core] = low

            @pl.when(at != tp)
            def _():
                sum_a[at] = low

            @pl.when(at == peer)
            def _():
                put(0, sum_a.at[at], 0, 0, at).start()

            @pl.when(step == 2)
            def _():
                relay(0, sum_a.at[at], at).start()

            @pl.when(step == 2 + onward)
            def _():
                put(0, sum_a.at[at], straight_slot, 0, at).start()

            @pl.when(step == 2 - onward)
            def _():
                own_a[at] = total
        else:
            total = own_b[at] + got_b[at].astype(F32)
            sum_b[at] = total.astype(BF16).reshape(8, 16, 384)
            own_b[at] = total
            relay(1, sum_b.at[at, pl.ds(place(2, 0), 2)], at).start()
            for c in (0, 1):
                put(1, sum_b.at[at, place(-onward, c)], straight_slot, at, place(-onward, c)).start()
            put(1, sum_b.at[at, peer], 0, at, peer).start()
            all_b[0, core, at] = sum_b[at, tp]

    def finish_one(group, at):
        if group == 0:
            @pl.when(lax.rem(at // 2 - chip + 4, 4) == 2 - onward)
            def _():
                relay(0, sum_a.at[at], at).wait_recv()
                sum_a[at] = (own_a[at] + via_a[at].reshape(128, 384).astype(F32)).astype(BF16).reshape(8, 16, 384)
                put(0, sum_a.at[at], added_slot, 0, at).start()
        else:
            first = place(onward, 0)
            relay(1, sum_b.at[at, pl.ds(0, 2)], at).wait_recv()
            rows = pl.ds(pl.multiple_of(first * 16, 32), 32)
            total = own_b[at, rows, :] + via_b[at].reshape(32, 384).astype(F32)
            sum_b[at, pl.ds(first, 2)] = total.astype(BF16).reshape(2, 16, 384)
            for c in (0, 1):
                put(1, sum_b.at[at, first + c], added_slot, at, first + c).start()

    def both_sides(act, away):
        for group, me in ((0, z), (1, y)):
            act(group, wrap(me + away))
            if 0 < away < 4:
                act(group, wrap(me - away))

    def combine(away):
        landed = got_a.at[pl.ds(0, 4 if 0 < away < 4 else 2)]
        pltpu.make_async_copy(landed, landed, pair_recv.at[away]).wait()
        both_sides(combine_one, away)

    def finish(away):
        both_sides(finish_one, away)

    def deep_pieces(which, away):
        for p in which:
            deep_piece(p, away)

    deep_hop(1, 1)
    deep_pieces((0, 2, 4, 6), 0)
    deep_hop(1, 2)
    deep_hop(1, 3)
    combine(0)
    deep_pieces((0, 1, 2, 3), 1)
    deep_hop(2, 0)
    deep_pieces((4, 5), 1)
    deep_hop(2, 1)
    deep_pieces((6, 7), 1)
    combine(1)
    deep_hop(2, 2)
    deep_hop(2, 3)
    finish(0)
    deep_pieces((0, 1, 2, 3), 2)
    deep_hop(3, 0)
    deep_pieces((4, 5, 6, 7), 2)
    deep_hop(3, 1)
    combine(2)
    deep_hop(3, 2)
    deep_hop(3, 3)
    finish(1)
    deep_pieces((0, 1, 2, 3, 4, 5, 6, 7), 3)
    combine(3)
    finish(2)
    deep_hop(4, 0)
    deep_pieces((0, 2, 4, 6), 4)
    combine(4)
    finish(3)
    finish(4)

    for c in range(2):
        for slot in range(3):
            wait_a = pltpu.make_async_copy(all_a.at[slot, c], all_a.at[slot, c], x_a_sem.at[slot, c]).wait
            wait_b = pltpu.make_async_copy(all_b.at[slot, c], all_b.at[slot, c], x_b_sem.at[slot, c]).wait
            if slot:
                wait_a()
                wait_b()
            else:
                pl.when(core != c)(wait_a)
                pl.when(core != c)(wait_b)

    for h, held in ((0, all_a), (1, all_b)):
        for c in range(2):
            total = held[0, c].astype(F32)
            for slot in range(1, 3):
                total += held[slot, c].astype(F32)
            flat[:, h, :, c * 384 : c * 384 + 384] = total
    scale = ds_in[...]
    for k in range(6):
        lanes = slice(k * 128, k * 128 + 128)
        block = flat[:, :, :, lanes].reshape(256, 128)
        out[lanes, :] = (block.T * scale).astype(BF16)

    for g in wide + deep:
        g.drain()
    for group, ref in ((0, give_a), (1, give_b)):
        pltpu.make_async_copy(ref, ref, pair_send.at[group]).wait()
    few = sum_a.at[pl.ds(0, 7)]
    pltpu.make_async_copy(few, few, x_send.at[0]).wait()
    few = sum_b.at[:, pl.ds(0, 7)]
    pltpu.make_async_copy(few, few, x_send.at[1]).wait()


def body(tokens, norm_gain, gate_weight, up_weight, gate_scale, up_scale, down_weight, down_scale):
    vmem = pl.BlockSpec(memory_space=pltpu.VMEM)
    hbm = pl.BlockSpec(memory_space=pl.ANY)
    dma = pltpu.SemaphoreType.DMA
    return pl.pallas_call(
        kernel,
        out_shape=jax.ShapeDtypeStruct((768, 256), BF16),
        in_specs=[hbm] * 8,
        out_specs=vmem,
        scratch_shapes=[
            pltpu.VMEM((768, 2048), BF16),
            pltpu.VMEM((32, 704), F32),
            pltpu.VMEM((32, 704), F32),
            pltpu.VMEM((32, 704), F32),
            pltpu.VMEM((1, 2048), F32),
            pltpu.VMEM((704,), F32),
            pltpu.VMEM((704,), F32),
            pltpu.VMEM((1, 256), F32),
            pltpu.VMEM((512, 512), BF16),
            pltpu.VMEM((2, 8, 768, 256), BF16),
            pltpu.VMEM((8, 8, 32, 768), BF16),
            pltpu.VMEM((8, 8, 32, 640), BF16),
            pltpu.VMEM((8, 8, 11, 8, 128), BF16),
            pltpu.VMEM((8, 8, 11, 8, 128), BF16),
            pltpu.VMEM((768, 768), F32),
            pltpu.VMEM((768, 640), F32),
            pltpu.VMEM((6, 768, 128), BF16),
            pltpu.VMEM((8, 128, 384), F32),
            pltpu.VMEM((8, 128, 384), F32),
            pltpu.VMEM((8, 128, 384), BF16),
            pltpu.VMEM((8, 128, 384), BF16),
            pltpu.VMEM((8, 128, 384), BF16),
            pltpu.VMEM((8, 128, 384), BF16),
            pltpu.VMEM((8, 8, 16, 384), BF16),
            pltpu.VMEM((8, 8, 16, 384), BF16),
            pltpu.VMEM((8, 8, 16, 384), BF16),
            pltpu.VMEM((8, 2, 16, 384), BF16),
            pltpu.VMEM((3, 2, 8, 16, 384), BF16),
            pltpu.VMEM((3, 2, 8, 16, 384), BF16),
            pltpu.VMEM((8, 2, 16, 768), F32),
            dma((8,)),
            dma((4,)),
            dma((4,)),
            dma((4, 2, 4)),
            dma((4, 26)),
            dma((2,)),
            dma((5,)),
            dma((8,)),
            dma((8,)),
            dma((2,)),
            dma((3, 2)),
            dma((3, 2)),
        ],
        compiler_params=pltpu.CompilerParams(
            collective_id=0, has_side_effects=True, vmem_limit_bytes=56 * 1024 * 1024
        ),
    )(
        tokens, norm_gain.reshape(1, 2048), gate_weight, up_weight, gate_scale, up_scale,
        down_weight.T, down_scale.reshape(1, 256),
    )


def solution(mesh):
    split = Mesh(mesh.devices.reshape(8, 8, mesh.shape["tp"]), ("fs_0", "fs_1", "tp"))
    placed = (P(FS, None), P(), P(FS, "tp"), P(FS, "tp"), P("tp"), P("tp"), P("tp", FS), P("tp"))
    return jax.shard_map(body, mesh=split, in_specs=placed, out_specs=P(FS, "tp"), check_vma=False)
```
